32 devices in a mesh: rep: 2 (over x), fs: 8 (over z, y), tp: 2 (over core).
Axes of the slice: x: 2, y: 2, z: 4, core: 2. Of those that a mesh axis runs over, the one named last changes fastest.
Arguments:
- tokens: bfloat16 [6144, 2048], P(('rep', 'fs', 'tp')), may hold values from -6 to 6
- mix_gain_in: float32 [2048], replicated, may hold values from 0.1 to 1.9
- pool_weight: bfloat16 [4, 512, 512], P(None, 'fs'), may hold values from -0.25 to 0.25
- mix_gain_out: float32 [2048], replicated, may hold values from 0.1 to 1.9
- ffn_gain_in: float32 [2048], replicated, may hold values from 0.1 to 1.9
- gate_weight: bfloat16 [2048, 5632], P('fs', 'tp'), may hold values from -0.125 to 0.125
- up_weight: bfloat16 [2048, 5632], P('fs', 'tp'), may hold values from -0.125 to 0.125
- gate_taps: float32 [3, 5632], replicated, may hold values from -3.5 to 3.5
- up_taps: float32 [3, 5632], replicated, may hold values from -3.5 to 3.5
- down_weight: bfloat16 [5632, 2048], P('tp', 'fs'), may hold values from -0.078125 to 0.078125
- ffn_gain_out: float32 [2048], replicated, may hold values from 0.1 to 1.9
Outputs:
- mixed_out: bfloat16 [6144, 2048], P(('rep', 'fs', 'tp'))
The draws below stay inside these ranges and needn't reach their ends.
All inputs are finite; a program needn't handle non-finite values.
Results may differ from the reference program's by a relative error of at most 0.014.
Values may be sent and summed in bfloat16 or wider, within the bound.
A program may use at most 128 MiB of HBM per device.

```python
import jax
import jax.numpy as jnp
from jax import lax

D = 2048
FF = 5632
GROUPS = 4
CONV_WIDTH = 3
GC = 512
SEQ_LEN = 384
SEQS = 16
TOKENS = 6144
N_TP = 2


def level_of(rng, dims, cuts, smallest, largest):
    level = 1.0
    for position, blocks in cuts:
        heights = jax.random.uniform(jax.random.fold_in(jax.random.fold_in(rng, 6), position), (blocks,), jnp.float32, smallest / len(cuts), largest / len(cuts))
        level = level * jnp.repeat(jnp.exp(heights), dims[position] // blocks).reshape((-1,) + (1,) * (len(dims) - 1 - position))
    return level


def bell_draw(own_key, dims, deviation, limit, cuts=(), kind=jnp.bfloat16):
    values = jax.random.normal(own_key, dims, jnp.float32) * deviation
    if len(cuts) > 0:
        values = level_of(own_key, dims, cuts, -0.22, 0.18) * values
    return jnp.clip(values, min=-limit, max=limit).astype(kind)


def setup_inputs(seed: int = 0) -> dict:
    key_of = jax.random.split(jax.random.key(seed), 12)
    return {
        "tokens": bell_draw(key_of[0], (TOKENS, D), 1.0, 6.0, ((0, 32),)),
        "mix_gain_in": jnp.clip(1.0 + 0.18 * jax.random.normal(key_of[1], (D,), jnp.float32), 0.1, 1.9),
        "pool_weight": bell_draw(key_of[2], (GROUPS, GC, GC), GC ** -0.5, 0.25, ((1, 8),)),
        "mix_gain_out": jnp.clip(1.0 + 0.18 * jax.random.normal(key_of[3], (D,), jnp.float32), 0.1, 1.9),
        "ffn_gain_in": jnp.clip(1.0 + 0.18 * jax.random.normal(key_of[4], (D,), jnp.float32), 0.1, 1.9),
        "gate_weight": bell_draw(key_of[5], (D, FF), D ** -0.5, 0.125, ((0, 8), (1, 2))),
        "up_weight": bell_draw(key_of[6], (D, FF), D ** -0.5, 0.125, ((0, 8), (1, 2))),
        "gate_taps": bell_draw(key_of[7], (CONV_WIDTH, FF), CONV_WIDTH ** -0.5, 3.5, (), jnp.float32),
        "up_taps": bell_draw(key_of[8], (CONV_WIDTH, FF), CONV_WIDTH ** -0.5, 3.5, (), jnp.float32),
        "down_weight": bell_draw(key_of[9], (FF, D), FF ** -0.5, 0.078125, ((0, 2), (1, 8))),
        "ffn_gain_out": jnp.clip(1.0 + 0.18 * jax.random.normal(key_of[10], (D,), jnp.float32), 0.1, 1.9),
    }


pool_spans = (2, 4, 8, 16)
rms_eps = 1e-06

def rms_scale(values, gain):
    floats = values.astype(jnp.float32)
    return floats * lax.rsqrt(lax.optimization_barrier(jnp.mean(floats * floats, axis=-1, keepdims=True)) + rms_eps) * gain.astype(jnp.float32)

def pooled_gap(padded, first, count):
    margin = padded.shape[0] - count
    floats = padded.astype(jnp.float32)
    width = padded.shape[1] // len(pool_spans)
    where = first + jnp.arange(count, dtype=jnp.int32)
    pieces = []
    for group, span in enumerate(pool_spans):
        block = floats[:, group * width:(group + 1) * width]
        total = jnp.zeros((count, width), jnp.float32)
        for back in range(span):
            total = total + block[margin - back:margin - back + count]
        divisor = jnp.minimum(where + 1, span).astype(jnp.float32)
        pieces.append(total / divisor[:, None] - block[margin:])
    return jnp.concatenate(pieces, axis=1).astype(jnp.bfloat16)

def causal_taps(pre, taps):
    width = taps.shape[0]
    floats = pre.astype(jnp.float32)
    padded = jnp.concatenate([jnp.zeros((width - 1, pre.shape[1]), jnp.float32), floats], axis=0)
    total = jnp.zeros(floats.shape, jnp.float32)
    for offset in range(width):
        total = total + taps[offset].astype(jnp.float32) * padded[offset:offset + pre.shape[0]]
    return total

def reference(tokens, mix_gain_in, pool_weight, mix_gain_out, ffn_gain_in, gate_weight, up_weight, gate_taps, up_taps, down_weight, ffn_gain_out):
    margin = max(pool_spans) - 1

    def one_sequence(rows):
        normed = rms_scale(rows, mix_gain_in).astype(jnp.bfloat16)
        padded = jnp.concatenate([jnp.zeros((margin, D), jnp.bfloat16), normed], axis=0)
        gap = pooled_gap(padded, 0, SEQ_LEN)
        mixed = jnp.einsum('rgc,gcj->rgj', gap.reshape(SEQ_LEN, GROUPS, GC).astype(jnp.float32), pool_weight.astype(jnp.float32))
        mixed = mixed.reshape(SEQ_LEN, D).astype(jnp.bfloat16)
        after_mix = rows.astype(jnp.float32) + rms_scale(mixed, mix_gain_out)
        channel_in = rms_scale(after_mix, ffn_gain_in).astype(jnp.bfloat16)
        gate_pre = jnp.dot(channel_in, gate_weight, preferred_element_type=jnp.float32).astype(jnp.bfloat16)
        up_pre = jnp.dot(channel_in, up_weight, preferred_element_type=jnp.float32).astype(jnp.bfloat16)
        gate_conv = causal_taps(gate_pre, gate_taps)
        up_conv = causal_taps(up_pre, up_taps)
        hidden = (jax.nn.gelu(gate_conv, approximate=True) * up_conv).astype(jnp.bfloat16)
        partial_value = jnp.einsum('rtf,tfd->rtd', hidden.reshape(SEQ_LEN, N_TP, FF // N_TP).astype(jnp.float32), down_weight.reshape(N_TP, FF // N_TP, D).astype(jnp.float32)).astype(jnp.bfloat16)
        channel_out = lax.optimization_barrier(jnp.sum(partial_value.astype(jnp.float32), axis=1))
        return (after_mix + rms_scale(channel_out, ffn_gain_out)).astype(jnp.bfloat16)
    result = lax.map(one_sequence, tokens.reshape(SEQS, SEQ_LEN, D))
    return result.reshape(TOKENS, D)
```

```python
import functools

import jax
import jax.numpy as jnp
from jax import lax
from jax.experimental import pallas as pl
from jax.experimental.pallas import tpu as pltpu
from jax.sharding import PartitionSpec as P

MESH = pl.DeviceIdType.MESH
pool_spans = (2, 4, 8, 16)
rms_eps = 1e-06
weight_budget = 24 * 2**20
f32 = jnp.float32
bf16 = jnp.bfloat16


def rms_scale(floats, gain):
    return floats * lax.rsqrt(jnp.mean(floats * floats, axis=-1, keepdims=True) + rms_eps) * gain


def gelu(v):
    return 0.5 * v * (1.0 + jnp.tanh(0.7978845608028654 * (v + 0.044715 * v * v * v)))


class Plan:
    def __init__(self, mesh, depth, width, columns):
        self.R, self.F, self.T = mesh.shape["rep"], mesh.shape["fs"], mesh.shape["tp"]
        self.Y = 1
        while 4 * self.Y * self.Y <= self.F:
            self.Y *= 2
        while self.F % self.Y:
            self.Y -= 1
        self.Z = self.F // self.Y
        self.joined = 3 * width * columns * 2 > weight_budget
        self.n_sub = self.R * self.Y if self.joined else 1
        self.G = self.T * self.n_sub
        self.cols = columns // self.n_sub

    def pool_owners(self, groups):
        S = min(self.T, groups)
        PR = self.R if self.joined and groups % (self.R * S) == 0 else 1
        return S, PR


def kernel(
    plan, tokens, gain_in, pool, gain_out, gain_ffn, gate_t, up_t, down_w, gate_taps, up_taps, gain_last, out,
    halo, pool_all, w_gu, w_d, x_all, normed, after, acc_g, acc_u, hidden, partial, swapped, summed, got,
    own_sem, halo_sem, y_ss, up_ss, dn_ss, piece_rs, pz_ss, pz_rs, pp_ss, pp_rs, share_ss, share_rs,
    x_ss, x_rs, f_ss, s_ss, s_rs, p_ss, p_rs,
):
    R, F, T, Y, Z, G, cols = plan.R, plan.F, plan.T, plan.Y, plan.Z, plan.G, plan.cols
    r, f, t = lax.axis_index("rep"), lax.axis_index("fs"), lax.axis_index("tp")
    z, y = f // Y, f % Y
    rows, width = tokens.shape
    depth = width // F
    groups, gc = pool_all.shape[0], pool_all.shape[3]
    slab = gc // F
    S, PR = plan.pool_owners(groups)
    PC = PR * Y
    GS = groups // (S * PR)
    q = t % S
    rp = r if PR > 1 else 0
    margin = halo.shape[0]
    C = G // T
    GA, UP, DN, POOL = 0, 1, 2, 3
    kinds = (GA, UP, DN)
    GU = (GA, UP)

    chip = r * Y + y if plan.joined else 0
    me = chip * T + t

    def peer(step):
        to = (chip + step) % C
        return {"rep": to // Y, "fs": z * Y + to % Y}

    def sub_of(y_to):
        return r * Y + y_to if plan.joined else 0

    def w_rows(y_to):
        return pl.ds(pl.multiple_of(sub_of(y_to) * cols, 64 if cols % 64 == 0 else 8), cols)

    def slot(kind, origin):
        return w_d.at[origin] if kind == DN else w_gu.at[origin, kind - GA]

    def source(kind, y_to):
        return (gate_t, up_t, down_w)[kind - GA].at[w_rows(y_to)]

    def pool_groups(rp_of, q_of):
        return pl.ds((rp_of * S + q_of) * GS, GS)

    def pool_rows(y_of):
        return pl.ds(pl.multiple_of(y_of * slab, slab), slab)

    def pool_own():
        return pltpu.make_async_copy(
            pool.at[pool_groups(rp, q)], pool_all.at[pool_groups(rp, q), z, pool_rows(y)], own_sem.at[POOL])

    def pool_z(step, z_from):
        return pltpu.make_async_remote_copy(
            src_ref=pool.at[pool_groups(rp, q)], dst_ref=pool_all.at[pool_groups(rp, q), z_from, pool_rows(y)],
            send_sem=pz_ss.at[step - 1], recv_sem=pz_rs.at[z_from],
            device_id={"fs": (z + step) % Z * Y + y}, device_id_type=MESH)

    def pool_plane(step, from_pc):
        block = pool_all.at[pool_groups(from_pc // Y, q), :, pool_rows(from_pc % Y)]
        to = (rp * Y + y + step) % PC
        device = {"fs": z * Y + to % Y}
        if PR > 1:
            device["rep"] = to // Y
        return pltpu.make_async_remote_copy(
            src_ref=block, dst_ref=block, send_sem=pp_ss.at[step - 1], recv_sem=pp_rs.at[from_pc],
            device_id=device, device_id_type=MESH)

    def share_copy(step, rp_of, q_from):
        block = pool_all.at[pool_groups(rp_of, q_from)]
        return pltpu.make_async_remote_copy(
            src_ref=block, dst_ref=block, send_sem=share_ss.at[step - 1, rp_of], recv_sem=share_rs.at[rp_of, q_from],
            device_id={"tp": t - q + (q + step) % S}, device_id_type=MESH)

    def own_copy(kind):
        return pltpu.make_async_copy(source(kind, y), slot(kind, f), own_sem.at[kind])

    def y_copy(kind, step):
        y_to = (y + step) % Y
        return pltpu.make_async_remote_copy(
            src_ref=source(kind, y_to), dst_ref=slot(kind, f), send_sem=y_ss.at[kind, step - 1],
            recv_sem=piece_rs.at[kind, f], device_id={"fs": z * Y + y_to}, device_id_type=MESH)

    def chain_copy(kind, origin, dz):
        return pltpu.make_async_remote_copy(
            src_ref=slot(kind, origin), dst_ref=slot(kind, origin), send_sem=(up_ss if dz > 0 else dn_ss).at[kind, origin],
            recv_sem=piece_rs.at[kind, origin], device_id={"fs": (z + dz) * Y + y}, device_id_type=MESH)

    def arrived(kind, origin):
        chain_copy(kind, origin, 1).wait_recv()

    def pass_on(kind, origin, z0):
        @pl.when((z0 <= z) & (z + 1 < Z))
        def _():
            chain_copy(kind, origin, 1).start()

        @pl.when((z0 >= z) & (z > 0))
        def _():
            chain_copy(kind, origin, -1).start()

    side = jnp.minimum(z, Z - 1 - z)

    def place(k):
        j = k // Y
        near = jnp.where(j % 2 == 1, z - (j + 1) // 2, z + j // 2)
        far = jnp.where(2 * z <= Z - 1, j, Z - 1 - j)
        z0 = jnp.where(j <= 2 * side, near, far)
        return z0, z0 * Y + (y + k % Y) % Y

    def chain(kinds_now, k):
        z0, origin = place(k)
        for kind in kinds_now:
            arrived(kind, origin)
            pass_on(kind, origin, z0)

    def chain_own(kinds_now):
        for kind in kinds_now:
            own_copy(kind).wait()
            pass_on(kind, f, z)

    def chain_range(kinds_now, first, last):
        def body(k, carry):
            chain(kinds_now, k)
            return carry
        lax.fori_loop(first, last, body, 0)

    def halo_copy():
        return pltpu.make_async_remote_copy(
            src_ref=tokens.at[pl.ds(rows - margin, margin)], dst_ref=halo, send_sem=halo_sem.at[0],
            recv_sem=halo_sem.at[1], device_id={"tp": (t + 1) % T}, device_id_type=MESH)

    def x_copy(step, c_from):
        g = c_from * T + t
        return pltpu.make_async_remote_copy(
            src_ref=x_all.at[g], dst_ref=x_all.at[g], send_sem=x_ss.at[step - 1],
            recv_sem=x_rs.at[g], device_id=peer(step), device_id_type=MESH)

    def x_across(step, c, t_from):
        g = c * T + t_from
        return pltpu.make_async_remote_copy(
            src_ref=x_all.at[g], dst_ref=x_all.at[g], send_sem=f_ss.at[step - 1, c],
            recv_sem=x_rs.at[g], device_id={"tp": (t + step) % T}, device_id_type=MESH)

    def s_copy(step, block, t_from):
        t_to = (t + step) % T
        return pltpu.make_async_remote_copy(
            src_ref=partial.at[block, t_to], dst_ref=swapped.at[block, t_from], send_sem=s_ss.at[block, step - 1],
            recv_sem=s_rs.at[block, t_from], device_id={"tp": t_to}, device_id_type=MESH)

    def p_copy(step, block, c_from):
        return pltpu.make_async_remote_copy(
            src_ref=summed.at[block, (chip + step) % C], dst_ref=got.at[block, c_from], send_sem=p_ss.at[block, step - 1],
            recv_sem=p_rs.at[block, c_from], device_id=peer(step), device_id_type=MESH)

    pool_own().start()
    for kind in kinds:
        own_copy(kind).start()
    near = [{"fs": (z + step) % Z * Y + y} for step in range(1, Z)]
    near += [peer(step) for step in range(1, C)] if plan.joined else [{"fs": z * Y + (y + step) % Y} for step in range(1, Y)]
    near += [{"tp": (t + step) % T} for step in range(1, T)]
    barrier = pltpu.get_barrier_semaphore()
    for device in near:
        pl.semaphore_signal(barrier, inc=1, device_id=device, device_id_type=MESH)
    pl.semaphore_wait(barrier, len(near))

    for step in range(1, Z):
        pool_z(step, z).start()
    halo_copy().start()
    for kind in GU:
        for step in range(1, Y):
            y_copy(kind, step).start()
    chain_own(GU)
    normed[pl.ds(margin, rows), :] = rms_scale(tokens[...].astype(f32), gain_in[...]).astype(bf16).astype(f32)
    halo_copy().wait_recv()
    before = rms_scale(halo[...].astype(f32), gain_in[...]).astype(bf16).astype(f32)
    normed[pl.ds(0, margin), :] = jnp.where(t > 0, before, 0.0)
    where = t * rows + lax.broadcasted_iota(jnp.int32, (rows, gc), 0)

    pool_own().wait()
    for step in range(1, Z):
        pool_z(step, (z + step) % Z).wait_recv()
    for step in range(1, PC):
        pool_plane(step, rp * Y + y).start()
    chain_range(GU, 1, Y)
    for step in range(1, PC):
        pool_plane(step, (rp * Y + y + step) % PC).wait_recv()
    for step in range(1, S):
        for rp_of in range(PR):
            share_copy(step, rp_of, q).start()
    for step in range(1, S):
        for rp_of in range(PR):
            share_copy(step, rp_of, (q + step) % S).wait_recv()
    for group, span in enumerate(pool_spans):
        total = normed[:, group * gc : (group + 1) * gc]
        block = total[margin:]
        reach = 1
        while reach < span:
            total = total + pltpu.roll(total, reach, 0)
            reach *= 2
        gap = (total[margin:] / jnp.minimum(where + 1, span).astype(f32) - block).astype(bf16)
        mixed = jnp.dot(gap, pool_all[group].reshape(gc, gc), preferred_element_type=f32)
        after[:, group * gc : (group + 1) * gc] = mixed.astype(bf16).astype(f32)
    after[...] = tokens[...].astype(f32) + rms_scale(after[...], gain_out[...])
    whole = rms_scale(after[...], gain_ffn[...]).astype(bf16)
    for k in range(F):
        x_all[me, k] = whole[:, k * depth : (k + 1) * depth]
    for step in range(1, C):
        x_copy(step, chip).start()
    for step in range(1, T):
        x_across(step, chip, t).start()

    acc_g[...] = jnp.zeros_like(acc_g)
    acc_u[...] = jnp.zeros_like(acc_u)

    def times(lhs, rhs):
        return lax.dot_general(lhs, rhs, (((1,), (1,)), ((), ())), preferred_element_type=f32)

    def gate_up(origin):
        def body(g, carry):
            x = x_all[g, origin]
            at = pl.ds(pl.multiple_of(8 + g * rows, 8), rows)
            acc_g[at, :] += times(x, w_gu[origin, 0])
            acc_u[at, :] += times(x, w_gu[origin, 1])
            return carry
        lax.fori_loop(0, G, body, 0)

    early = jnp.where(side > 0, F, Y)
    ahead = Y * (1 + 2 * side)
    for step in range(1, Y):
        y_copy(DN, step).start()
    chain_range(GU, Y, early)
    chain_own((DN,))
    chain_range((DN,), 1, Y)
    for back in range(1, C):
        c = (chip + C - back) % C
        x_copy(back, c).wait_recv()
        for step in range(1, T):
            x_across(step, c, t).start()
    for c in range(C):
        for step in range(1, T):
            x_across(step, c, (t + step) % T).wait_recv()

    def gate_up_step(k, carry):
        @pl.when(k >= early)
        def _():
            chain(GU, k)
        gate_up(place(k)[1])
        return carry
    lax.fori_loop(0, F, gate_up_step, 0)
    chain_range((DN,), Y, ahead)

    taps = gate_taps.shape[0]

    def convolve(acc, taps_ref, g, keep):
        block = acc[pl.ds(pl.multiple_of(g * rows, 8), rows + 8), :]
        total = taps_ref[taps - 1 : taps, :] * block[8:]
        for back in range(1, taps):
            moved = pltpu.roll(block, back, 0)[8:]
            total = total + taps_ref[taps - 1 - back : taps - back, :] * jnp.where(keep >= back, moved, 0.0)
        return total

    def activate(g, carry):
        keep = (g % T) * rows + lax.broadcasted_iota(jnp.int32, (rows, cols), 0)
        hidden[g] = (gelu(convolve(acc_g, gate_taps, g, keep)) * convolve(acc_u, up_taps, g, keep)).astype(bf16)
        return carry

    lax.fori_loop(0, G, activate, 0)

    def down(block):
        def body(i, carry):
            step, c = i // C + 1, i % C
            t_to = (t + step) % T
            product = jnp.dot(hidden[c * T + t_to], w_d[block], preferred_element_type=f32)
            partial[block, t_to, c] = product.astype(bf16)
            return carry
        lax.fori_loop(0, G - C, body, 0)
        for step in range(1, T):
            s_copy(step, block, t).start()
        lax.fori_loop(G - C, G, body, 0)

    def add_up(block):
        for back in range(1, T):
            s_copy(back, block, (t + back) % T).wait_recv()

        def body(c, carry):
            total = partial[block, t, c].astype(f32)
            for back in range(1, T):
                total = total + swapped[block, (t + back) % T, c].astype(f32)
            summed[block, c] = total.astype(bf16)
            return carry
        lax.fori_loop(0, C, body, 0)
        for step in range(1, C):
            p_copy(step, block, chip).start()
        got[block, chip] = summed[block, chip]

    def down_step(k, carry):
        @pl.when(k >= ahead)
        def _():
            add_up(place(k - 1)[1])
            chain((DN,), k)
        down(place(k)[1])

        @pl.when((k > 0) & (k < ahead))
        def _():
            add_up(place(k - 1)[1])
        return carry
    lax.fori_loop(0, F, down_step, 0)
    add_up(place(F - 1)[1])

    def finish(block, carry):
        for step in range(1, C):
            p_copy(step, block, (chip + step) % C).wait_recv()
        return carry

    lax.fori_loop(0, F, finish, 0)
    for k in range(F):
        total = got[k, 0].astype(f32)
        for c in range(1, C):
            total = total + got[k, c].astype(f32)
        normed[pl.ds(0, rows), k * depth : (k + 1) * depth] = total
    out[...] = (after[...] + rms_scale(normed[pl.ds(0, rows), :], gain_last[...])).astype(bf16)

    halo_copy().wait_send()
    for step in range(1, Z):
        pool_z(step, z).wait_send()
    for step in range(1, PC):
        pool_plane(step, rp * Y + y).wait_send()
    for step in range(1, S):
        for rp_of in range(PR):
            share_copy(step, rp_of, q).wait_send()
    for step in range(1, C):
        x_copy(step, chip).wait_send()
    for step in range(1, T):
        for c in range(C):
            x_across(step, c, t).wait_send()
    for kind in kinds:
        for step in range(1, Y):
            y_copy(kind, step).wait_send()

        def ended(origin, carry):
            @pl.when((origin // Y <= z) & (z + 1 < Z))
            def _():
                chain_copy(kind, origin, 1).wait_send()

            @pl.when((origin // Y >= z) & (z > 0))
            def _():
                chain_copy(kind, origin, -1).wait_send()
            return carry
        lax.fori_loop(0, F, ended, 0)

    def sent(block, carry):
        for step in range(1, T):
            s_copy(step, block, t).wait_send()
        for step in range(1, C):
            p_copy(step, block, chip).wait_send()
        return carry
    lax.fori_loop(0, F, sent, 0)


def solution(mesh):
    def shards(tokens, gain_in, pool, gain_out, gain_ffn, gate_w, up_w, gate_taps, up_taps, down_w, gain_last):
        rows, width = tokens.shape
        depth, columns = gate_w.shape
        plan = Plan(mesh, depth, width, columns)
        F, G, T, Y, Z, cols = plan.F, plan.G, plan.T, plan.Y, plan.Z, plan.cols
        groups, gc = pool.shape[0], pool.shape[2]
        C = G // T
        first = lax.axis_index("tp") * columns
        if plan.joined:
            first = first + (lax.axis_index("rep") * Y + lax.axis_index("fs") % Y) * cols
        gt = lax.dynamic_slice_in_dim(gate_taps, first, cols, 1)
        ut = lax.dynamic_slice_in_dim(up_taps, first, cols, 1)
        margin = max(pool_spans)
        vmem = pl.BlockSpec(memory_space=pltpu.VMEM)
        anywhere = pl.BlockSpec(memory_space=pl.ANY)
        dma = pltpu.SemaphoreType.DMA
        S, PR = plan.pool_owners(groups)
        PC = PR * Y
        V = pltpu.VMEM
        return pl.pallas_call(
            functools.partial(kernel, plan),
            out_shape=jax.ShapeDtypeStruct((rows, width), bf16),
            in_specs=[vmem, vmem, anywhere, vmem, vmem, anywhere, anywhere, anywhere, vmem, vmem, vmem],
            out_specs=vmem,
            scratch_shapes=[
                V((margin, width), bf16), V((groups, Z, gc // Z, gc), bf16), V((F, 2, cols, depth), bf16), V((F, cols, depth), bf16),
                V((G, F, rows, depth), bf16), V((margin + rows, width), f32), V((rows, width), f32),
                V((8 + G * rows, cols), f32), V((8 + G * rows, cols), f32), V((G, rows, cols), bf16),
                V((F, T, C, rows, depth), bf16), V((F, T, C, rows, depth), bf16), V((F, C, rows, depth), bf16), V((F, C, rows, depth), bf16),
                dma((4,)), dma((2,)), dma((3, max(Y - 1, 1))), dma((3, F)), dma((3, F)), dma((3, F)),
                dma((max(Z - 1, 1),)), dma((Z,)), dma((max(PC - 1, 1),)), dma((PC,)), dma((max(S - 1, 1), PR)), dma((PR, S)), dma((max(C - 1, 1),)), dma((G,)),
                dma((max(T - 1, 1), C)), dma((F, max(T - 1, 1))), dma((F, T)), dma((F, max(C - 1, 1))), dma((F, C)),
            ],
            compiler_params=pltpu.CompilerParams(has_side_effects=True, collective_id=0, vmem_limit_bytes=61 * 2**20),
            name="layer",
        )(tokens, gain_in[None], pool, gain_out[None], gain_ffn[None], gate_w.T, up_w.T, down_w, gt, ut, gain_last[None])

    in_specs = (
        P(("rep", "fs", "tp"), None), P(), P(None, "fs", None), P(), P(),
        P("fs", "tp"), P("fs", "tp"), P(), P(), P("tp", "fs"), P(),
    )
    return jax.shard_map(shards, mesh=mesh, in_specs=in_specs, out_specs=P(("rep", "fs", "tp"), None), check_vma=False)
```

```python
import functools

import jax
import jax.numpy as jnp
from jax import lax
from jax.experimental import pallas as pl
from jax.experimental.pallas import tpu as pltpu
from jax.sharding import PartitionSpec as P

MESH = pl.DeviceIdType.MESH
pool_spans = (2, 4, 8, 16)
rms_eps = 1e-06
lanes = 128
weight_budget = 24 * 2**20
f32 = jnp.float32
bf16 = jnp.bfloat16


def rms_scale(floats, gain):
    return floats * lax.rsqrt(jnp.mean(floats * floats, axis=-1, keepdims=True) + rms_eps) * gain


def gelu(v):
    return 0.5 * v * (1.0 + jnp.tanh(0.7978845608028654 * (v + 0.044715 * v * v * v)))


class Plan:
    def __init__(self, mesh, depth, width, columns):
        self.R, self.F, self.T = mesh.shape["rep"], mesh.shape["fs"], mesh.shape["tp"]
        self.Y = 1
        while 4 * self.Y * self.Y <= self.F:
            self.Y *= 2
        while self.F % self.Y:
            self.Y -= 1
        self.Z = self.F // self.Y
        self.joined = 3 * width * columns * 2 > weight_budget and columns % lanes == 0
        self.n_sub = self.R * self.Y if self.joined else 1
        self.G = self.T * self.n_sub
        self.tiles = columns // lanes
        self.cols = -(-self.tiles // self.n_sub) * lanes if self.joined else columns
        self.small = self.tiles // self.n_sub * lanes if self.joined else columns

    def first_tile(self, sub, t):
        return (sub * self.tiles + self.n_sub // 2 * ((t + 1) % 2)) // self.n_sub

    def pool_owners(self, groups):
        S = min(self.T, groups)
        PR = self.R if self.joined and groups % (self.R * S) == 0 else 1
        return S, PR


def kernel(
    plan, tokens, gain_in, pool, gain_out, gain_ffn, gate_w, up_w, down_w, gate_taps, up_taps, gain_last, out,
    halo, pool_all, w_gu, w_d, x_all, normed, after, acc_g, acc_u, hidden, partial, swapped, summed, got,
    own_sem, halo_sem, y_ss, up_ss, dn_ss, piece_rs, pz_ss, pz_rs, pp_ss, pp_rs, share_ss, share_rs,
    x_ss, x_rs, f_ss, s_ss, s_rs, p_ss, p_rs,
):
    R, F, T, Y, Z, G, cols = plan.R, plan.F, plan.T, plan.Y, plan.Z, plan.G, plan.cols
    r, f, t = lax.axis_index("rep"), lax.axis_index("fs"), lax.axis_index("tp")
    z, y = f // Y, f % Y
    rows, width = tokens.shape
    depth = width // F
    groups, gc = pool_all.shape[0], pool_all.shape[3]
    slab = gc // F
    S, PR = plan.pool_owners(groups)
    PC = PR * Y
    GS = groups // (S * PR)
    q = t % S
    rp = r if PR > 1 else 0
    margin = halo.shape[0]
    C = G // T
    GA, UP, DN, POOL = 0, 1, 2, 3
    kinds = (GA, UP, DN)
    GU = (GA, UP)

    chip = r * Y + y if plan.joined else 0
    me = chip * T + t

    def peer(step):
        to = (chip + step) % C
        return {"rep": to // Y, "fs": z * Y + to % Y}

    def sub_of(y_to):
        return r * Y + y_to if plan.joined else 0

    def by_size(y_to, run):
        if plan.small == cols:
            run(cols)
            return
        tiles = plan.first_tile(sub_of(y_to) + 1, t) - plan.first_tile(sub_of(y_to), t)

        @pl.when(tiles * lanes == cols)
        def _():
            run(cols)

        @pl.when(tiles * lanes != cols)
        def _():
            run(plan.small)

    def columns_of(y_to, size):
        if not plan.joined:
            return pl.ds(0, size)
        return pl.ds(pl.multiple_of(plan.first_tile(sub_of(y_to), t) * lanes, lanes), size)

    def slot(kind, origin, size):
        return w_d.at[origin, pl.ds(0, size)] if kind == DN else w_gu.at[origin, kind - GA, :, pl.ds(0, size)]

    def source(kind, y_to, size):
        if kind == DN:
            return down_w.at[columns_of(y_to, size)]
        return (gate_w, up_w)[kind - GA].at[:, columns_of(y_to, size)]

    def pool_groups(rp_of, q_of):
        return pl.ds((rp_of * S + q_of) * GS, GS)

    def pool_rows(y_of):
        return pl.ds(pl.multiple_of(y_of * slab, slab), slab)

    def pool_own():
        return pltpu.make_async_copy(
            pool.at[pool_groups(rp, q)], pool_all.at[pool_groups(rp, q), z, pool_rows(y)], own_sem.at[POOL])

    def pool_z(step, z_from):
        return pltpu.make_async_remote_copy(
            src_ref=pool.at[pool_groups(rp, q)], dst_ref=pool_all.at[pool_groups(rp, q), z_from, pool_rows(y)],
            send_sem=pz_ss.at[step - 1], recv_sem=pz_rs.at[z_from],
            device_id={"fs": (z + step) % Z * Y + y}, device_id_type=MESH)

    def pool_plane(step, from_pc):
        block = pool_all.at[pool_groups(from_pc // Y, q), :, pool_rows(from_pc % Y)]
        to = (rp * Y + y + step) % PC
        device = {"fs": z * Y + to % Y}
        if PR > 1:
            device["rep"] = to // Y
        return pltpu.make_async_remote_copy(
            src_ref=block, dst_ref=block, send_sem=pp_ss.at[step - 1], recv_sem=pp_rs.at[from_pc],
            device_id=device, device_id_type=MESH)

    def share_copy(step, rp_of, q_from):
        block = pool_all.at[pool_groups(rp_of, q_from)]
        return pltpu.make_async_remote_copy(
            src_ref=block, dst_ref=block, send_sem=share_ss.at[step - 1, rp_of], recv_sem=share_rs.at[rp_of, q_from],
            device_id={"tp": t - q + (q + step) % S}, device_id_type=MESH)

    def own_copy(kind, size):
        return pltpu.make_async_copy(source(kind, y, size), slot(kind, f, size), own_sem.at[kind])

    def y_copy(kind, step, size):
        y_to = (y + step) % Y
        return pltpu.make_async_remote_copy(
            src_ref=source(kind, y_to, size), dst_ref=slot(kind, f, size), send_sem=y_ss.at[kind, step - 1],
            recv_sem=piece_rs.at[kind, f], device_id={"fs": z * Y + y_to}, device_id_type=MESH)

    def chain_copy(kind, origin, dz, size):
        block = slot(kind, origin, size)
        return pltpu.make_async_remote_copy(
            src_ref=block, dst_ref=block, send_sem=(up_ss if dz > 0 else dn_ss).at[kind, origin],
            recv_sem=piece_rs.at[kind, origin], device_id={"fs": (z + dz) * Y + y}, device_id_type=MESH)

    def pass_on(kind, origin, z0, size):
        @pl.when((z0 <= z) & (z + 1 < Z))
        def _():
            chain_copy(kind, origin, 1, size).start()

        @pl.when((z0 >= z) & (z > 0))
        def _():
            chain_copy(kind, origin, -1, size).start()

    def y_start(kinds_now):
        for step in range(1, Y):
            by_size((y + step) % Y, lambda size: [y_copy(kind, step, size).start() for kind in kinds_now])

    side = jnp.minimum(z, Z - 1 - z)

    def place(k):
        j = k // Y
        near = jnp.where(j % 2 == 1, z - (j + 1) // 2, z + j // 2)
        far = jnp.where(2 * z <= Z - 1, j, Z - 1 - j)
        z0 = jnp.where(j <= 2 * side, near, far)
        return z0, z0 * Y + (y + k % Y) % Y

    def chain(kinds_now, k):
        z0, origin = place(k)

        def run(size):
            for kind in kinds_now:
                chain_copy(kind, origin, 1, size).wait_recv()
                pass_on(kind, origin, z0, size)
        by_size(y, run)

    def chain_own(kinds_now):
        def run(size):
            for kind in kinds_now:
                own_copy(kind, size).wait()
                pass_on(kind, f, z, size)
        by_size(y, run)

    def chain_range(kinds_now, first, last):
        def body(k, carry):
            chain(kinds_now, k)
            return carry
        lax.fori_loop(first, last, body, 0)

    def halo_copy():
        return pltpu.make_async_remote_copy(
            src_ref=tokens.at[pl.ds(rows - margin, margin)], dst_ref=halo, send_sem=halo_sem.at[0],
            recv_sem=halo_sem.at[1], device_id={"tp": (t + 1) % T}, device_id_type=MESH)

    def x_copy(step, c_from):
        g = c_from * T + t
        return pltpu.make_async_remote_copy(
            src_ref=x_all.at[g], dst_ref=x_all.at[g], send_sem=x_ss.at[step - 1],
            recv_sem=x_rs.at[g], device_id=peer(step), device_id_type=MESH)

    def x_across(step, c, t_from):
        g = c * T + t_from
        return pltpu.make_async_remote_copy(
            src_ref=x_all.at[g], dst_ref=x_all.at[g], send_sem=f_ss.at[step - 1, c],
            recv_sem=x_rs.at[g], device_id={"tp": (t + step) % T}, device_id_type=MESH)

    def s_copy(step, block, t_from):
        t_to = (t + step) % T
        return pltpu.make_async_remote_copy(
            src_ref=partial.at[block, t_to], dst_ref=swapped.at[block, step - 1], send_sem=s_ss.at[block, step - 1],
            recv_sem=s_rs.at[block, t_from], device_id={"tp": t_to}, device_id_type=MESH)

    def p_copy(step, block, c_from):
        return pltpu.make_async_remote_copy(
            src_ref=summed.at[block, (chip + step) % C], dst_ref=got.at[block, c_from], send_sem=p_ss.at[block, step - 1],
            recv_sem=p_rs.at[block, c_from], device_id=peer(step), device_id_type=MESH)

    pool_own().start()
    by_size(y, lambda size: [own_copy(kind, size).start() for kind in kinds])
    near = [{"fs": (z + step) % Z * Y + y} for step in range(1, Z)]
    near += [peer(step) for step in range(1, C)] if plan.joined else [{"fs": z * Y + (y + step) % Y} for step in range(1, Y)]
    near += [{"tp": (t + step) % T} for step in range(1, T)]
    barrier = pltpu.get_barrier_semaphore()
    for device in near:
        pl.semaphore_signal(barrier, inc=1, device_id=device, device_id_type=MESH)
    def blank(size):
        if size < cols:
            w_gu[:, :, :, size:cols] = jnp.zeros((F, 2, depth, cols - size), bf16)
            w_d[:, size:cols] = jnp.zeros((F, cols - size, depth), bf16)
    by_size(y, blank)
    pl.semaphore_wait(barrier, len(near))

    for step in range(1, Z):
        pool_z(step, z).start()
    halo_copy().start()
    y_start(GU)
    chain_own(GU)
    normed[pl.ds(margin, rows), :] = rms_scale(tokens[...].astype(f32), gain_in[...]).astype(bf16).astype(f32)
    halo_copy().wait_recv()
    before = rms_scale(halo[...].astype(f32), gain_in[...]).astype(bf16).astype(f32)
    normed[pl.ds(0, margin), :] = jnp.where(t > 0, before, 0.0)
    where = t * rows + lax.broadcasted_iota(jnp.int32, (rows, gc), 0)

    pool_own().wait()
    for step in range(1, Z):
        pool_z(step, (z + step) % Z).wait_recv()
    for step in range(1, PC):
        pool_plane(step, rp * Y + y).start()
    chain_range(GU, 1, Y)
    for step in range(1, PC):
        pool_plane(step, (rp * Y + y + step) % PC).wait_recv()
    for step in range(1, S):
        for rp_of in range(PR):
            share_copy(step, rp_of, q).start()
    for step in range(1, S):
        for rp_of in range(PR):
            share_copy(step, rp_of, (q + step) % S).wait_recv()
    for group, span in enumerate(pool_spans):
        total = normed[:, group * gc : (group + 1) * gc]
        block = total[margin:]
        reach = 1
        while reach < span:
            total = total + pltpu.roll(total, reach, 0)
            reach *= 2
        gap = (total[margin:] / jnp.minimum(where + 1, span).astype(f32) - block).astype(bf16)
        mixed = jnp.dot(gap, pool_all[group].reshape(gc, gc), preferred_element_type=f32)
        after[:, group * gc : (group + 1) * gc] = mixed.astype(bf16).astype(f32)
    after[...] = tokens[...].astype(f32) + rms_scale(after[...], gain_out[...])
    whole = rms_scale(after[...], gain_ffn[...]).astype(bf16)
    for k in range(F):
        x_all[me, k] = whole[:, k * depth : (k + 1) * depth]
    for step in range(1, C):
        x_copy(step, chip).start()
    for step in range(1, T):
        x_across(step, chip, t).start()

    acc_g[...] = jnp.zeros_like(acc_g)
    acc_u[...] = jnp.zeros_like(acc_u)

    def times(lhs, rhs):
        return jnp.dot(lhs, rhs, preferred_element_type=f32)

    def gate_up(origin):
        def body(g, carry):
            x = x_all[g, origin]
            at = pl.ds(pl.multiple_of(8 + g * rows, 8), rows)
            acc_g[at, :] += times(x, w_gu[origin, 0])
            acc_u[at, :] += times(x, w_gu[origin, 1])
            return carry
        lax.fori_loop(0, G, body, 0)

    early = jnp.where(side > 0, F, Y)
    ahead = Y * (1 + 2 * side)
    y_start((DN,))
    chain_range(GU, Y, early)
    chain_own((DN,))
    chain_range((DN,), 1, Y)
    for back in range(1, C):
        c = (chip + C - back) % C
        x_copy(back, c).wait_recv()
        for step in range(1, T):
            x_across(step, c, t).start()
    for c in range(C):
        for step in range(1, T):
            x_across(step, c, (t + step) % T).wait_recv()

    def gate_up_step(k, carry):
        @pl.when(k >= early)
        def _():
            chain(GU, k)
        gate_up(place(k)[1])
        return carry
    lax.fori_loop(0, F, gate_up_step, 0)
    chain_range((DN,), Y, ahead)

    taps = gate_taps.shape[0]
    window = pl.ds(pl.multiple_of(t * plan.tiles * lanes + plan.first_tile(sub_of(y), t) * lanes, lanes), cols) if plan.joined else slice(None)

    def convolve(acc, taps_ref, g, keep):
        block = acc[pl.ds(pl.multiple_of(g * rows, 8), rows + 8), :]
        total = taps_ref[taps - 1 : taps, window] * block[8:]
        for back in range(1, taps):
            moved = pltpu.roll(block, back, 0)[8:]
            total = total + taps_ref[taps - 1 - back : taps - back, window] * jnp.where(keep >= back, moved, 0.0)
        return total

    def activate(g, carry):
        keep = (g % T) * rows + lax.broadcasted_iota(jnp.int32, (rows, cols), 0)
        hidden[g] = (gelu(convolve(acc_g, gate_taps, g, keep)) * convolve(acc_u, up_taps, g, keep)).astype(bf16)
        return carry

    lax.fori_loop(0, G, activate, 0)

    def down(block):
        def body(i, carry):
            step, c = i // C + 1, i % C
            t_to = (t + step) % T
            product = jnp.dot(hidden[c * T + t_to], w_d[block], preferred_element_type=f32)
            partial[block, t_to, c] = product.astype(bf16)
            return carry
        lax.fori_loop(0, G - C, body, 0)
        for step in range(1, T):
            s_copy(step, block, t).start()
        lax.fori_loop(G - C, G, body, 0)

    def add_up(block):
        for back in range(1, T):
            s_copy(back, block, (t + back) % T).wait_recv()

        def body(c, carry):
            total = partial[block, t, c].astype(f32)
            for back in range(1, T):
                total = total + swapped[block, T - 1 - back, c].astype(f32)
            summed[block, c] = total.astype(bf16)
            return carry
        lax.fori_loop(0, C, body, 0)
        for step in range(1, C):
            p_copy(step, block, chip).start()
        got[block, chip] = summed[block, chip]

    def down_step(k, carry):
        @pl.when(k >= ahead)
        def _():
            add_up(place(k - 1)[1])
            chain((DN,), k)
        down(place(k)[1])

        @pl.when((k > 0) & (k < ahead))
        def _():
            add_up(place(k - 1)[1])
        return carry
    lax.fori_loop(0, F, down_step, 0)
    add_up(place(F - 1)[1])

    def finish(block, carry):
        for step in range(1, C):
            p_copy(step, block, (chip + step) % C).wait_recv()
        return carry

    lax.fori_loop(0, F, finish, 0)
    for k in range(F):
        total = got[k, 0].astype(f32)
        for c in range(1, C):
            total = total + got[k, c].astype(f32)
        normed[pl.ds(0, rows), k * depth : (k + 1) * depth] = total
    out[...] = (after[...] + rms_scale(normed[pl.ds(0, rows), :], gain_last[...])).astype(bf16)

    halo_copy().wait_send()
    for step in range(1, Z):
        pool_z(step, z).wait_send()
    for step in range(1, PC):
        pool_plane(step, rp * Y + y).wait_send()
    for step in range(1, S):
        for rp_of in range(PR):
            share_copy(step, rp_of, q).wait_send()
    for step in range(1, C):
        x_copy(step, chip).wait_send()
    for step in range(1, T):
        for c in range(C):
            x_across(step, c, t).wait_send()
    for step in range(1, Y):
        by_size((y + step) % Y, lambda size: [y_copy(kind, step, size).wait_send() for kind in kinds])

    def all_ended(size):
        for kind in kinds:
            def ended(origin, carry):
                @pl.when((origin // Y <= z) & (z + 1 < Z))
                def _():
                    chain_copy(kind, origin, 1, size).wait_send()

                @pl.when((origin // Y >= z) & (z > 0))
                def _():
                    chain_copy(kind, origin, -1, size).wait_send()
                return carry
            lax.fori_loop(0, F, ended, 0)
    by_size(y, all_ended)

    def sent(block, carry):
        for step in range(1, T):
            s_copy(step, block, t).wait_send()
        for step in range(1, C):
            p_copy(step, block, chip).wait_send()
        return carry
    lax.fori_loop(0, F, sent, 0)


def solution(mesh):
    def shards(tokens, gain_in, pool, gain_out, gain_ffn, gate_w, up_w, gate_taps, up_taps, down_w, gain_last):
        rows, width = tokens.shape
        depth, columns = gate_w.shape
        plan = Plan(mesh, depth, width, columns)
        F, G, T, Y, Z, cols = plan.F, plan.G, plan.T, plan.Y, plan.Z, plan.cols
        groups, gc = pool.shape[0], pool.shape[2]
        C = G // T
        gt, ut = gate_taps, up_taps
        if not plan.joined:
            gt, ut = (lax.dynamic_slice_in_dim(v, lax.axis_index("tp") * columns, columns, 1) for v in (gate_taps, up_taps))
        margin = max(pool_spans)
        vmem = pl.BlockSpec(memory_space=pltpu.VMEM)
        anywhere = pl.BlockSpec(memory_space=pl.ANY)
        dma = pltpu.SemaphoreType.DMA
        S, PR = plan.pool_owners(groups)
        PC = PR * Y
        V = pltpu.VMEM
        return pl.pallas_call(
            functools.partial(kernel, plan),
            out_shape=jax.ShapeDtypeStruct((rows, width), bf16),
            in_specs=[vmem, vmem, anywhere, vmem, vmem, anywhere, anywhere, anywhere, vmem, vmem, vmem],
            out_specs=vmem,
            scratch_shapes=[
                V((margin, width), bf16), V((groups, Z, gc // Z, gc), bf16), V((F, 2, depth, cols), bf16), V((F, cols, depth), bf16),
                V((G, F, rows, depth), bf16), V((margin + rows, width), f32), V((rows, width), f32),
                V((8 + G * rows, cols), f32), V((8 + G * rows, cols), f32), V((G, rows, cols), bf16),
                V((F, T, C, rows, depth), bf16), V((F, max(T - 1, 1), C, rows, depth), bf16), V((F, C, rows, depth), bf16), V((F, C, rows, depth), bf16),
                dma((4,)), dma((2,)), dma((3, max(Y - 1, 1))), dma((3, F)), dma((3, F)), dma((3, F)),
                dma((max(Z - 1, 1),)), dma((Z,)), dma((max(PC - 1, 1),)), dma((PC,)), dma((max(S - 1, 1), PR)), dma((PR, S)), dma((max(C - 1, 1),)), dma((G,)),
                dma((max(T - 1, 1), C)), dma((F, max(T - 1, 1))), dma((F, T)), dma((F, max(C - 1, 1))), dma((F, C)),
            ],
            compiler_params=pltpu.CompilerParams(has_side_effects=True, collective_id=0, vmem_limit_bytes=52 * 2**20),
            name="layer",
        )(tokens, gain_in[None], pool, gain_out[None], gain_ffn[None], gate_w, up_w, down_w, gt, ut, gain_last[None])

    in_specs = (
        P(("rep", "fs", "tp"), None), P(), P(None, "fs", None), P(), P(),
        P("fs", "tp"), P("fs", "tp"), P(), P(), P("tp", "fs"), P(),
    )
    return jax.shard_map(shards, mesh=mesh, in_specs=in_specs, out_specs=P(("rep", "fs", "tp"), None), check_vma=False)
```

```python
import functools

import jax
import jax.numpy as jnp
from jax import lax
from jax.experimental import pallas as pl
from jax.experimental.pallas import tpu as pltpu
from jax.sharding import PartitionSpec as P

MESH = pl.DeviceIdType.MESH
pool_spans = (2, 4, 8, 16)
rms_eps = 1e-06
lanes = 128
weight_budget = 24 * 2**20
f32 = jnp.float32
bf16 = jnp.bfloat16


def rms_scale(floats, gain):
    return floats * lax.rsqrt(jnp.mean(floats * floats, axis=-1, keepdims=True) + rms_eps) * gain


def gelu(v):
    return 0.5 * v * (1.0 + jnp.tanh(0.7978845608028654 * (v + 0.044715 * v * v * v)))


class Plan:
    def __init__(self, mesh, depth, width, columns):
        self.R, self.F, self.T = mesh.shape["rep"], mesh.shape["fs"], mesh.shape["tp"]
        self.Y = 1
        while 4 * self.Y * self.Y <= self.F:
            self.Y *= 2
        while self.F % self.Y:
            self.Y -= 1
        self.Z = self.F // self.Y
        self.joined = 3 * width * columns * 2 > weight_budget and columns % lanes == 0
        self.n_sub = self.R * self.Y if self.joined else 1
        self.G = self.T * self.n_sub
        self.tiles = columns // lanes
        self.cols = -(-self.tiles // self.n_sub) * lanes if self.joined else columns
        self.small = self.tiles // self.n_sub * lanes if self.joined else columns

    def halves(self, depth):
        return 2 if depth % (2 * lanes) == 0 else 1

    def first_tile(self, sub, t):
        return (sub * self.tiles + self.n_sub // 2 * ((t + 1) % 2)) // self.n_sub

    def pool_owners(self, groups):
        S = min(self.T, groups)
        PR = self.R if self.joined and groups % (self.R * S) == 0 else 1
        return S, PR


def kernel(
    plan, tokens_hbm, gain_in_hbm, pool, gain_out_hbm, gain_ffn_hbm, gate_w, up_w, down_w, gate_taps_hbm, up_taps_hbm, gain_last_hbm, out,
    tokens, gain_in, gain_out, gain_ffn, gate_taps, up_taps, gain_last,
    halo, pool_all, w_gu, w_d, x_all, normed, after, acc_g, acc_u, hidden, partial, swapped, summed, got,
    in_sem, own_sem, halo_sem, y_ss, up_ss, dn_ss, piece_rs, pz_ss, pz_rs, pp_ss, pp_rs, share_ss, share_rs,
    x_ss, x_rs, f_ss, s_ss, s_rs, p_ss, p_rs,
):
    R, F, T, Y, Z, G, cols = plan.R, plan.F, plan.T, plan.Y, plan.Z, plan.G, plan.cols
    r, f, t = lax.axis_index("rep"), lax.axis_index("fs"), lax.axis_index("tp")
    z, y = f // Y, f % Y
    rows, width = tokens.shape
    depth = width // F
    groups, gc = pool_all.shape[0], pool_all.shape[3]
    slab = gc // F
    S, PR = plan.pool_owners(groups)
    PC = PR * Y
    GS = groups // (S * PR)
    q = t % S
    rp = r if PR > 1 else 0
    margin = halo.shape[0]
    C = G // T
    H = plan.halves(depth)
    half = depth // H
    GA, UP, DN = 0, 1, 2
    GU = (GA, UP)
    DNS = tuple(range(DN, DN + H))
    kinds = GU + DNS
    POOL = DN + H

    chip = r * Y + y if plan.joined else 0
    me = chip * T + t

    def peer(step):
        to = (chip + step) % C
        return {"rep": to // Y, "fs": z * Y + to % Y}

    def sub_of(y_to):
        return r * Y + y_to if plan.joined else 0

    def by_size(y_to, run):
        if plan.small == cols:
            run(cols)
            return
        tiles = plan.first_tile(sub_of(y_to) + 1, t) - plan.first_tile(sub_of(y_to), t)

        @pl.when(tiles * lanes == cols)
        def _():
            run(cols)

        @pl.when(tiles * lanes != cols)
        def _():
            run(plan.small)

    def columns_of(y_to, size):
        if not plan.joined:
            return pl.ds(0, size)
        return pl.ds(pl.multiple_of(plan.first_tile(sub_of(y_to), t) * lanes, lanes), size)

    def part(h):
        return pl.ds(0, depth) if h is None else pl.ds(h * half, half)

    def slot(kind, origin, size):
        if kind in DNS:
            return w_d.at[origin, pl.ds(0, size), part(kind - DN)]
        return w_gu.at[origin, kind - GA, :, pl.ds(0, size)]

    def source(kind, y_to, size):
        if kind in DNS:
            return down_w.at[columns_of(y_to, size), part(kind - DN)]
        return (gate_w, up_w)[kind - GA].at[:, columns_of(y_to, size)]

    def pool_groups(rp_of, q_of):
        return pl.ds((rp_of * S + q_of) * GS, GS)

    def pool_rows(y_of):
        return pl.ds(pl.multiple_of(y_of * slab, slab), slab)

    def pool_own():
        return pltpu.make_async_copy(
            pool.at[pool_groups(rp, q)], pool_all.at[pool_groups(rp, q), z, pool_rows(y)], own_sem.at[POOL])

    def pool_z(step, z_from):
        return pltpu.make_async_remote_copy(
            src_ref=pool.at[pool_groups(rp, q)], dst_ref=pool_all.at[pool_groups(rp, q), z_from, pool_rows(y)],
            send_sem=pz_ss.at[step - 1], recv_sem=pz_rs.at[z_from],
            device_id={"fs": (z + step) % Z * Y + y}, device_id_type=MESH)

    def pool_plane(step, from_pc):
        block = pool_all.at[pool_groups(from_pc // Y, q), :, pool_rows(from_pc % Y)]
        to = (rp * Y + y + step) % PC
        device = {"fs": z * Y + to % Y}
        if PR > 1:
            device["rep"] = to // Y
        return pltpu.make_async_remote_copy(
            src_ref=block, dst_ref=block, send_sem=pp_ss.at[step - 1], recv_sem=pp_rs.at[from_pc],
            device_id=device, device_id_type=MESH)

    def share_copy(step, rp_of, q_from):
        block = pool_all.at[pool_groups(rp_of, q_from)]
        return pltpu.make_async_remote_copy(
            src_ref=block, dst_ref=block, send_sem=share_ss.at[step - 1, rp_of], recv_sem=share_rs.at[rp_of, q_from],
            device_id={"tp": t - q + (q + step) % S}, device_id_type=MESH)

    def own_copy(kind, size):
        return pltpu.make_async_copy(source(kind, y, size), slot(kind, f, size), own_sem.at[kind])

    def y_copy(kind, step, size):
        y_to = (y + step) % Y
        return pltpu.make_async_remote_copy(
            src_ref=source(kind, y_to, size), dst_ref=slot(kind, f, size), send_sem=y_ss.at[kind, step - 1],
            recv_sem=piece_rs.at[kind, f], device_id={"fs": z * Y + y_to}, device_id_type=MESH)

    def chain_copy(kind, origin, dz, size):
        block = slot(kind, origin, size)
        return pltpu.make_async_remote_copy(
            src_ref=block, dst_ref=block, send_sem=(up_ss if dz > 0 else dn_ss).at[kind, origin],
            recv_sem=piece_rs.at[kind, origin], device_id={"fs": (z + dz) * Y + y}, device_id_type=MESH)

    def pass_on(kind, origin, z0, size):
        @pl.when((z0 <= z) & (z + 1 < Z))
        def _():
            chain_copy(kind, origin, 1, size).start()

        @pl.when((z0 >= z) & (z > 0))
        def _():
            chain_copy(kind, origin, -1, size).start()

    def y_start(kinds_now):
        for step in range(1, Y):
            by_size((y + step) % Y, lambda size: [y_copy(kind, step, size).start() for kind in kinds_now])

    side = jnp.minimum(z, Z - 1 - z)

    def place(k):
        j = k // Y
        near = jnp.where(j % 2 == 1, z - (j + 1) // 2, z + j // 2)
        far = jnp.where(2 * z <= Z - 1, j, Z - 1 - j)
        z0 = jnp.where(j <= 2 * side, near, far)
        return z0, z0 * Y + (y + k % Y) % Y

    def chain(kinds_now, k):
        z0, origin = place(k)

        def run(size):
            for kind in kinds_now:
                chain_copy(kind, origin, 1, size).wait_recv()
                pass_on(kind, origin, z0, size)
        by_size(y, run)

    def chain_own(kinds_now):
        def run(size):
            for kind in kinds_now:
                own_copy(kind, size).wait()
                pass_on(kind, f, z, size)
        by_size(y, run)

    def chain_range(kinds_now, first, last):
        def body(k, carry):
            chain(kinds_now, k)
            return carry
        lax.fori_loop(first, last, body, 0)

    def halo_copy():
        return pltpu.make_async_remote_copy(
            src_ref=tokens_hbm.at[pl.ds(rows - margin, margin)], dst_ref=halo, send_sem=halo_sem.at[0],
            recv_sem=halo_sem.at[1], device_id={"tp": (t + 1) % T}, device_id_type=MESH)

    def x_copy(step, c_from):
        g = c_from * T + t
        return pltpu.make_async_remote_copy(
            src_ref=x_all.at[g], dst_ref=x_all.at[g], send_sem=x_ss.at[step - 1],
            recv_sem=x_rs.at[g], device_id=peer(step), device_id_type=MESH)

    def x_across(step, c, t_from):
        g = c * T + t_from
        return pltpu.make_async_remote_copy(
            src_ref=x_all.at[g], dst_ref=x_all.at[g], send_sem=f_ss.at[step - 1, c],
            recv_sem=x_rs.at[g], device_id={"tp": (t + step) % T}, device_id_type=MESH)

    def flag(block, h):
        return block if h is None else F + h

    def s_copy(step, block, t_from, h=None):
        t_to = (t + step) % T
        return pltpu.make_async_remote_copy(
            src_ref=partial.at[block, t_to, :, :, part(h)], dst_ref=swapped.at[block, step - 1, :, :, part(h)],
            send_sem=s_ss.at[flag(block, h), step - 1], recv_sem=s_rs.at[flag(block, h), t_from],
            device_id={"tp": t_to}, device_id_type=MESH)

    def p_copy(step, block, c_from, h=None):
        return pltpu.make_async_remote_copy(
            src_ref=summed.at[block, (chip + step) % C, :, part(h)], dst_ref=got.at[block, c_from, :, part(h)],
            send_sem=p_ss.at[flag(block, h), step - 1], recv_sem=p_rs.at[flag(block, h), c_from],
            device_id=peer(step), device_id_type=MESH)

    def last_block(y_of):
        return place(F - 1)[0] * Y + (y_of + (F - 1) % Y) % Y

    staged = [
        pltpu.make_async_copy(source_ref, held, in_sem.at[k]) for k, (source_ref, held) in enumerate((
            (tokens_hbm, tokens), (gain_in_hbm, gain_in), (gain_out_hbm, gain_out), (gain_ffn_hbm, gain_ffn),
            (gate_taps_hbm, gate_taps), (up_taps_hbm, up_taps), (gain_last_hbm, gain_last)))]
    staged[0].start()
    staged[1].start()
    pool_own().start()
    by_size(y, lambda size: [own_copy(kind, size).start() for kind in kinds])
    near = [{"fs": (z + step) % Z * Y + y} for step in range(1, Z)]
    near += [peer(step) for step in range(1, C)] if plan.joined else [{"fs": z * Y + (y + step) % Y} for step in range(1, Y)]
    near += [{"tp": (t + step) % T} for step in range(1, T)]
    barrier = pltpu.get_barrier_semaphore()
    for device in near:
        pl.semaphore_signal(barrier, inc=1, device_id=device, device_id_type=MESH)
    def blank(size):
        if size < cols:
            w_gu[:, :, :, size:cols] = jnp.zeros((F, 2, depth, cols - size), bf16)
            w_d[:, size:cols] = jnp.zeros((F, cols - size, depth), bf16)
    by_size(y, blank)
    pl.semaphore_wait(barrier, len(near))

    for step in range(1, Z):
        pool_z(step, z).start()
    halo_copy().start()
    y_start(GU)
    chain_own(GU)
    for copy in staged[2:]:
        copy.start()
    for copy in staged:
        copy.wait()
    normed[pl.ds(margin, rows), :] = rms_scale(tokens[...].astype(f32), gain_in[...]).astype(bf16).astype(f32)
    halo_copy().wait_recv()
    before = rms_scale(halo[...].astype(f32), gain_in[...]).astype(bf16).astype(f32)
    normed[pl.ds(0, margin), :] = jnp.where(t > 0, before, 0.0)
    where = t * rows + lax.broadcasted_iota(jnp.int32, (rows, gc), 0)

    pool_own().wait()
    for step in range(1, Z):
        pool_z(step, (z + step) % Z).wait_recv()
    for step in range(1, PC):
        pool_plane(step, rp * Y + y).start()
    chain_range(GU, 1, Y)
    for step in range(1, PC):
        pool_plane(step, (rp * Y + y + step) % PC).wait_recv()
    for step in range(1, S):
        for rp_of in range(PR):
            share_copy(step, rp_of, q).start()
    for step in range(1, S):
        for rp_of in range(PR):
            share_copy(step, rp_of, (q + step) % S).wait_recv()
    for group, span in enumerate(pool_spans):
        total = normed[:, group * gc : (group + 1) * gc]
        block = total[margin:]
        reach = 1
        while reach < span:
            total = total + pltpu.roll(total, reach, 0)
            reach *= 2
        gap = (total[margin:] / jnp.minimum(where + 1, span).astype(f32) - block).astype(bf16)
        mixed = jnp.dot(gap, pool_all[group].reshape(gc, gc), preferred_element_type=f32)
        after[:, group * gc : (group + 1) * gc] = mixed.astype(bf16).astype(f32)
    after[...] = tokens[...].astype(f32) + rms_scale(after[...], gain_out[...])
    whole = rms_scale(after[...], gain_ffn[...]).astype(bf16)
    for k in range(F):
        x_all[me, k] = whole[:, k * depth : (k + 1) * depth]
    for step in range(1, C):
        x_copy(step, chip).start()
    for step in range(1, T):
        x_across(step, chip, t).start()

    acc_g[...] = jnp.zeros_like(acc_g)
    acc_u[...] = jnp.zeros_like(acc_u)

    def times(lhs, rhs):
        return jnp.dot(lhs, rhs, preferred_element_type=f32)

    def gate_up(origin):
        def body(g, carry):
            x = x_all[g, origin]
            at = pl.ds(pl.multiple_of(8 + g * rows, 8), rows)
            acc_g[at, :] += times(x, w_gu[origin, 0])
            acc_u[at, :] += times(x, w_gu[origin, 1])
            return carry
        lax.fori_loop(0, G, body, 0)

    early = jnp.where(side > 0, F, Y)
    ahead = Y * (1 + 2 * side)
    y_start(DNS)
    chain_range(GU, Y, early)
    chain_own(DNS)
    chain_range(DNS, 1, Y)
    for back in range(1, C):
        c = (chip + C - back) % C
        x_copy(back, c).wait_recv()
        for step in range(1, T):
            x_across(step, c, t).start()
    for c in range(C):
        for step in range(1, T):
            x_across(step, c, (t + step) % T).wait_recv()

    def gate_up_step(k, carry):
        @pl.when(k >= early)
        def _():
            chain(GU, k)
        gate_up(place(k)[1])
        return carry
    lax.fori_loop(0, F, gate_up_step, 0)
    chain_range(DNS, Y, jnp.minimum(ahead, F - 1))

    taps = gate_taps.shape[0]
    window = pl.ds(pl.multiple_of(t * plan.tiles * lanes + plan.first_tile(sub_of(y), t) * lanes, lanes), cols) if plan.joined else slice(None)

    def convolve(acc, taps_ref, g, keep):
        block = acc[pl.ds(pl.multiple_of(g * rows, 8), rows + 8), :]
        total = taps_ref[taps - 1 : taps, window] * block[8:]
        for back in range(1, taps):
            moved = pltpu.roll(block, back, 0)[8:]
            total = total + taps_ref[taps - 1 - back : taps - back, window] * jnp.where(keep >= back, moved, 0.0)
        return total

    def activate(g, carry):
        keep = (g % T) * rows + lax.broadcasted_iota(jnp.int32, (rows, cols), 0)
        hidden[g] = (gelu(convolve(acc_g, gate_taps, g, keep)) * convolve(acc_u, up_taps, g, keep)).astype(bf16)
        return carry

    lax.fori_loop(0, G, activate, 0)

    def down(block, h=None):
        def body(i, carry):
            step, c = i // C + 1, i % C
            t_to = (t + step) % T
            product = jnp.dot(hidden[c * T + t_to], w_d[block, :, part(h)], preferred_element_type=f32)
            partial[block, t_to, c, :, part(h)] = product.astype(bf16)
            return carry
        lax.fori_loop(0, G - C, body, 0)
        for step in range(1, T):
            s_copy(step, block, t, h).start()
        lax.fori_loop(G - C, G, body, 0)

    def add_up(block, h=None):
        for back in range(1, T):
            s_copy(back, block, (t + back) % T, h).wait_recv()

        def body(c, carry):
            total = partial[block, t, c, :, part(h)].astype(f32)
            for back in range(1, T):
                total = total + swapped[block, T - 1 - back, c, :, part(h)].astype(f32)
            summed[block, c, :, part(h)] = total.astype(bf16)
            return carry
        lax.fori_loop(0, C, body, 0)
        for step in range(1, C):
            p_copy(step, block, chip, h).start()
        got[block, chip, :, part(h)] = summed[block, chip, :, part(h)]

    def down_step(k, carry):
        @pl.when(k >= ahead)
        def _():
            add_up(place(k - 1)[1])
            chain(DNS, k)
        down(place(k)[1])

        @pl.when((k > 0) & (k < ahead))
        def _():
            add_up(place(k - 1)[1])
        return carry
    lax.fori_loop(0, F - 1, down_step, 0)
    if F > 1:
        add_up(place(F - 2)[1])
    for h in range(H):
        if F > Y:
            chain((DNS[h],), F - 1)
        down(last_block(y), h)
        add_up(last_block(y), h)

    def finish(block, carry):
        for step in range(1, C):
            @pl.when(block != last_block((chip + step) % C % Y))
            def _():
                p_copy(step, block, (chip + step) % C).wait_recv()
        return carry

    lax.fori_loop(0, F, finish, 0)
    for step in range(1, C):
        for h in range(H):
            c_from = (chip + step) % C
            p_copy(step, last_block(c_from % Y), c_from, h).wait_recv()
    for k in range(F):
        total = got[k, 0].astype(f32)
        for c in range(1, C):
            total = total + got[k, c].astype(f32)
        normed[pl.ds(0, rows), k * depth : (k + 1) * depth] = total
    out[...] = (after[...] + rms_scale(normed[pl.ds(0, rows), :], gain_last[...])).astype(bf16)

    halo_copy().wait_send()
    for step in range(1, Z):
        pool_z(step, z).wait_send()
    for step in range(1, PC):
        pool_plane(step, rp * Y + y).wait_send()
    for step in range(1, S):
        for rp_of in range(PR):
            share_copy(step, rp_of, q).wait_send()
    for step in range(1, C):
        x_copy(step, chip).wait_send()
    for step in range(1, T):
        for c in range(C):
            x_across(step, c, t).wait_send()
    for step in range(1, Y):
        by_size((y + step) % Y, lambda size: [y_copy(kind, step, size).wait_send() for kind in kinds])

    def all_ended(size):
        for kind in kinds:
            def ended(origin, carry):
                @pl.when((origin // Y <= z) & (z + 1 < Z))
                def _():
                    chain_copy(kind, origin, 1, size).wait_send()

                @pl.when((origin // Y >= z) & (z > 0))
                def _():
                    chain_copy(kind, origin, -1, size).wait_send()
                return carry
            lax.fori_loop(0, F, ended, 0)
    by_size(y, all_ended)

    def sent(block, carry):
        @pl.when(block != last_block(y))
        def _():
            for step in range(1, T):
                s_copy(step, block, t).wait_send()
            for step in range(1, C):
                p_copy(step, block, chip).wait_send()
        return carry
    lax.fori_loop(0, F, sent, 0)
    for h in range(H):
        for step in range(1, T):
            s_copy(step, last_block(y), t, h).wait_send()
        for step in range(1, C):
            p_copy(step, last_block(y), chip, h).wait_send()


def solution(mesh):
    def shards(tokens, gain_in, pool, gain_out, gain_ffn, gate_w, up_w, gate_taps, up_taps, down_w, gain_last):
        rows, width = tokens.shape
        depth, columns = gate_w.shape
        plan = Plan(mesh, depth, width, columns)
        F, G, T, Y, Z, cols = plan.F, plan.G, plan.T, plan.Y, plan.Z, plan.cols
        groups, gc = pool.shape[0], pool.shape[2]
        C = G // T
        gt, ut = gate_taps, up_taps
        if not plan.joined:
            gt, ut = (lax.dynamic_slice_in_dim(v, lax.axis_index("tp") * columns, columns, 1) for v in (gate_taps, up_taps))
        margin = max(pool_spans)
        vmem = pl.BlockSpec(memory_space=pltpu.VMEM)
        dma = pltpu.SemaphoreType.DMA
        S, PR = plan.pool_owners(groups)
        PC = PR * Y
        H = plan.halves(depth)
        K = 2 + H
        V = pltpu.VMEM
        return pl.pallas_call(
            functools.partial(kernel, plan),
            out_shape=pltpu.VMEM((rows, width), bf16),
            in_specs=[pl.BlockSpec(memory_space=pltpu.HBM)] * 11,
            out_specs=vmem,
            scratch_shapes=[
                V((rows, width), bf16), V((1, width), f32), V((1, width), f32), V((1, width), f32), V(gt.shape, f32), V(ut.shape, f32), V((1, width), f32),
                V((margin, width), bf16), V((groups, Z, gc // Z, gc), bf16), V((F, 2, depth, cols), bf16), V((F, cols, depth), bf16),
                V((G, F, rows, depth), bf16), V((margin + rows, width), f32), V((rows, width), f32),
                V((8 + G * rows, cols), f32), V((8 + G * rows, cols), f32), V((G, rows, cols), bf16),
                V((F, T, C, rows, depth), bf16), V((F, max(T - 1, 1), C, rows, depth), bf16), V((F, C, rows, depth), bf16), V((F, C, rows, depth), bf16),
                dma((7,)), dma((K + 1,)), dma((2,)), dma((K, max(Y - 1, 1))), dma((K, F)), dma((K, F)), dma((K, F)),
                dma((max(Z - 1, 1),)), dma((Z,)), dma((max(PC - 1, 1),)), dma((PC,)), dma((max(S - 1, 1), PR)), dma((PR, S)), dma((max(C - 1, 1),)), dma((G,)),
                dma((max(T - 1, 1), C)), dma((F + H, max(T - 1, 1))), dma((F + H, T)), dma((F + H, max(C - 1, 1))), dma((F + H, C)),
            ],
            compiler_params=pltpu.CompilerParams(has_side_effects=True, collective_id=0, vmem_limit_bytes=54 * 2**20),
            name="layer",
        )(tokens, gain_in[None], pool, gain_out[None], gain_ffn[None], gate_w, up_w, down_w, gt, ut, gain_last[None])

    in_specs = (
        P(("rep", "fs", "tp"), None), P(), P(None, "fs", None), P(), P(),
        P("fs", "tp"), P("fs", "tp"), P(), P(), P("tp", "fs"), P(),
    )
    return jax.shard_map(shards, mesh=mesh, in_specs=in_specs, out_specs=P(("rep", "fs", "tp"), None), check_vma=False)
```

```python
import functools

import jax
import jax.numpy as jnp
from jax import lax
from jax.experimental import pallas as pl
from jax.experimental.pallas import tpu as pltpu
from jax.sharding import PartitionSpec as P

MESH = pl.DeviceIdType.MESH
pool_spans = (2, 4, 8, 16)
rms_eps = 1e-06
lanes = 128
weight_budget = 24 * 2**20
f32 = jnp.float32
bf16 = jnp.bfloat16


def rms_scale(floats, gain):
    return floats * lax.rsqrt(jnp.mean(floats * floats, axis=-1, keepdims=True) + rms_eps) * gain


def gelu(v):
    return 0.5 * v * (1.0 + jnp.tanh(0.7978845608028654 * (v + 0.044715 * v * v * v)))


class Plan:
    def __init__(self, mesh, depth, width, columns):
        self.R, self.F, self.T = mesh.shape["rep"], mesh.shape["fs"], mesh.shape["tp"]
        self.Y = 1
        while 4 * self.Y * self.Y <= self.F:
            self.Y *= 2
        while self.F % self.Y:
            self.Y -= 1
        self.Z = self.F // self.Y
        self.joined = 3 * width * columns * 2 > weight_budget and columns % lanes == 0
        self.n_sub = self.R * self.Y if self.joined else 1
        self.G = self.T * self.n_sub
        self.tiles = columns // lanes
        self.cols = -(-self.tiles // self.n_sub) * lanes if self.joined else columns
        self.small = self.tiles // self.n_sub * lanes if self.joined else columns

    def halves(self, depth):
        return 2 if depth % (2 * lanes) == 0 else 1

    def first_tile(self, sub, t):
        return (sub * self.tiles + self.n_sub // 2 * ((t + 1) % 2)) // self.n_sub

    def pool_owners(self, groups):
        S = min(self.T, groups)
        PR = self.R if self.joined and groups % (self.R * S) == 0 else 1
        return S, PR


def kernel(
    plan, tokens_hbm, gain_in_hbm, pool, gain_out_hbm, gain_ffn_hbm, gate_w, up_w, down_w, gate_taps_hbm, up_taps_hbm, gain_last_hbm, out,
    tokens, gain_in, gain_out, gain_ffn, gate_taps, up_taps, gain_last,
    halo, pool_all, w_gu, w_d, x_all, normed, after, acc_g, acc_u, hidden, partial, swapped, summed, got,
    in_sem, own_sem, halo_sem, y_ss, up_ss, dn_ss, piece_rs, pz_ss, pz_rs, pp_ss, pp_rs, share_ss, share_rs,
    x_ss, x_rs, f_ss, s_ss, s_rs, p_ss, p_rs,
):
    R, F, T, Y, Z, G, cols = plan.R, plan.F, plan.T, plan.Y, plan.Z, plan.G, plan.cols
    r, f, t = lax.axis_index("rep"), lax.axis_index("fs"), lax.axis_index("tp")
    z, y = f // Y, f % Y
    rows, width = tokens.shape
    depth = width // F
    groups, gc = pool_all.shape[0], pool_all.shape[3]
    slab = gc // F
    S, PR = plan.pool_owners(groups)
    PC = PR * Y
    GS = groups // (S * PR)
    q = t % S
    rp = r if PR > 1 else 0
    margin = halo.shape[0]
    C = G // T
    H = plan.halves(depth)
    half = depth // H
    GA, UP, DN = 0, 1, 2
    GU = (GA, UP)
    DNS = tuple(range(DN, DN + H))
    kinds = GU + DNS
    POOL = DN + H

    chip = r * Y + y if plan.joined else 0
    me = chip * T + t

    def peer(step):
        to = (chip + step) % C
        return {"rep": to // Y, "fs": z * Y + to % Y}

    def sub_of(y_to):
        return r * Y + y_to if plan.joined else 0

    def by_size(y_to, run):
        if plan.small == cols:
            run(cols)
            return
        tiles = plan.first_tile(sub_of(y_to) + 1, t) - plan.first_tile(sub_of(y_to), t)

        @pl.when(tiles * lanes == cols)
        def _():
            run(cols)

        @pl.when(tiles * lanes != cols)
        def _():
            run(plan.small)

    def columns_of(y_to, size):
        if not plan.joined:
            return pl.ds(0, size)
        return pl.ds(pl.multiple_of(plan.first_tile(sub_of(y_to), t) * lanes, lanes), size)

    def part(h):
        return pl.ds(0, depth) if h is None else pl.ds(h * half, half)

    def slot(kind, origin, size):
        if kind in DNS:
            return w_d.at[origin, pl.ds(0, size), part(kind - DN)]
        return w_gu.at[origin, kind - GA, :, pl.ds(0, size)]

    def source(kind, y_to, size):
        if kind in DNS:
            return down_w.at[columns_of(y_to, size), part(kind - DN)]
        return (gate_w, up_w)[kind - GA].at[:, columns_of(y_to, size)]

    def pool_groups(rp_of, q_of):
        return pl.ds((rp_of * S + q_of) * GS, GS)

    def pool_rows(y_of):
        return pl.ds(pl.multiple_of(y_of * slab, slab), slab)

    def pool_own():
        return pltpu.make_async_copy(
            pool.at[pool_groups(rp, q)], pool_all.at[pool_groups(rp, q), z, pool_rows(y)], own_sem.at[POOL])

    def pool_z(step, z_from):
        return pltpu.make_async_remote_copy(
            src_ref=pool.at[pool_groups(rp, q)], dst_ref=pool_all.at[pool_groups(rp, q), z_from, pool_rows(y)],
            send_sem=pz_ss.at[step - 1], recv_sem=pz_rs.at[z_from],
            device_id={"fs": (z + step) % Z * Y + y}, device_id_type=MESH)

    def pool_plane(step, from_pc):
        block = pool_all.at[pool_groups(from_pc // Y, q), :, pool_rows(from_pc % Y)]
        to = (rp * Y + y + step) % PC
        device = {"fs": z * Y + to % Y}
        if PR > 1:
            device["rep"] = to // Y
        return pltpu.make_async_remote_copy(
            src_ref=block, dst_ref=block, send_sem=pp_ss.at[step - 1], recv_sem=pp_rs.at[from_pc],
            device_id=device, device_id_type=MESH)

    def share_copy(step, rp_of, q_from):
        block = pool_all.at[pool_groups(rp_of, q_from)]
        return pltpu.make_async_remote_copy(
            src_ref=block, dst_ref=block, send_sem=share_ss.at[step - 1, rp_of], recv_sem=share_rs.at[rp_of, q_from],
            device_id={"tp": t - q + (q + step) % S}, device_id_type=MESH)

    def own_copy(kind, size):
        return pltpu.make_async_copy(source(kind, y, size), slot(kind, f, size), own_sem.at[kind])

    def y_copy(kind, step, size):
        y_to = (y + step) % Y
        return pltpu.make_async_remote_copy(
            src_ref=source(kind, y_to, size), dst_ref=slot(kind, f, size), send_sem=y_ss.at[kind, step - 1],
            recv_sem=piece_rs.at[kind, f], device_id={"fs": z * Y + y_to}, device_id_type=MESH)

    def chain_copy(kind, origin, dz, size):
        block = slot(kind, origin, size)
        return pltpu.make_async_remote_copy(
            src_ref=block, dst_ref=block, send_sem=(up_ss if dz > 0 else dn_ss).at[kind, origin],
            recv_sem=piece_rs.at[kind, origin], device_id={"fs": (z + dz) * Y + y}, device_id_type=MESH)

    def pass_on(kind, origin, z0, size):
        @pl.when((z0 <= z) & (z + 1 < Z))
        def _():
            chain_copy(kind, origin, 1, size).start()

        @pl.when((z0 >= z) & (z > 0))
        def _():
            chain_copy(kind, origin, -1, size).start()

    def y_start(kinds_now):
        for step in range(1, Y):
            by_size((y + step) % Y, lambda size: [y_copy(kind, step, size).start() for kind in kinds_now])

    side = jnp.minimum(z, Z - 1 - z)

    def place(k):
        j = k // Y
        near = jnp.where(j % 2 == 1, z - (j + 1) // 2, z + j // 2)
        far = jnp.where(2 * z <= Z - 1, j, Z - 1 - j)
        z0 = jnp.where(j <= 2 * side, near, far)
        return z0, z0 * Y + (y + k % Y) % Y

    def chain(kinds_now, k):
        z0, origin = place(k)

        def run(size):
            for kind in kinds_now:
                chain_copy(kind, origin, 1, size).wait_recv()
                pass_on(kind, origin, z0, size)
        by_size(y, run)

    def chain_own(kinds_now):
        def run(size):
            for kind in kinds_now:
                own_copy(kind, size).wait()
                pass_on(kind, f, z, size)
        by_size(y, run)

    def chain_range(kinds_now, first, last):
        def body(k, carry):
            chain(kinds_now, k)
            return carry
        lax.fori_loop(first, last, body, 0)

    def halo_copy():
        return pltpu.make_async_remote_copy(
            src_ref=tokens_hbm.at[pl.ds(rows - margin, margin)], dst_ref=halo, send_sem=halo_sem.at[0],
            recv_sem=halo_sem.at[1], device_id={"tp": (t + 1) % T}, device_id_type=MESH)

    def x_copy(step, c_from):
        g = c_from * T + t
        return pltpu.make_async_remote_copy(
            src_ref=x_all.at[g], dst_ref=x_all.at[g], send_sem=x_ss.at[step - 1],
            recv_sem=x_rs.at[g], device_id=peer(step), device_id_type=MESH)

    def x_across(step, c, t_from):
        g = c * T + t_from
        return pltpu.make_async_remote_copy(
            src_ref=x_all.at[g], dst_ref=x_all.at[g], send_sem=f_ss.at[step - 1, c],
            recv_sem=x_rs.at[g], device_id={"tp": (t + step) % T}, device_id_type=MESH)

    def flag(block, h):
        return block if h is None else F + h

    def s_copy(step, block, t_from, c, h=None):
        t_to = (t + step) % T
        return pltpu.make_async_remote_copy(
            src_ref=partial.at[block, t_to, c, :, part(h)], dst_ref=swapped.at[block, step - 1, c, :, part(h)],
            send_sem=s_ss.at[flag(block, h), step - 1, c], recv_sem=s_rs.at[flag(block, h), t_from, c],
            device_id={"tp": t_to}, device_id_type=MESH)

    def p_copy(step, block, c_from, h=None):
        return pltpu.make_async_remote_copy(
            src_ref=summed.at[block, (chip + step) % C, :, part(h)], dst_ref=got.at[block, c_from, :, part(h)],
            send_sem=p_ss.at[flag(block, h), step - 1], recv_sem=p_rs.at[flag(block, h), c_from],
            device_id=peer(step), device_id_type=MESH)

    def last_block(y_of):
        return place(F - 1)[0] * Y + (y_of + (F - 1) % Y) % Y

    staged = [
        pltpu.make_async_copy(source_ref, held, in_sem.at[k]) for k, (source_ref, held) in enumerate((
            (tokens_hbm, tokens), (gain_in_hbm, gain_in), (gain_out_hbm, gain_out), (gain_ffn_hbm, gain_ffn),
            (gate_taps_hbm, gate_taps), (up_taps_hbm, up_taps), (gain_last_hbm, gain_last)))]
    staged[0].start()
    staged[1].start()
    pool_own().start()
    by_size(y, lambda size: [own_copy(kind, size).start() for kind in kinds])
    near = [{"fs": (z + step) % Z * Y + y} for step in range(1, Z)]
    near += [peer(step) for step in range(1, C)] if plan.joined else [{"fs": z * Y + (y + step) % Y} for step in range(1, Y)]
    near += [{"tp": (t + step) % T} for step in range(1, T)]
    barrier = pltpu.get_barrier_semaphore()
    for device in near:
        pl.semaphore_signal(barrier, inc=1, device_id=device, device_id_type=MESH)
    def blank(size):
        if size < cols:
            w_gu[:, :, :, size:cols] = jnp.zeros((F, 2, depth, cols - size), bf16)
            w_d[:, size:cols] = jnp.zeros((F, cols - size, depth), bf16)
    by_size(y, blank)
    pl.semaphore_wait(barrier, len(near))

    for step in range(1, Z):
        pool_z(step, z).start()
    halo_copy().start()
    y_start(GU)
    chain_own(GU)
    for copy in staged[2:]:
        copy.start()
    for copy in staged:
        copy.wait()
    normed[pl.ds(margin, rows), :] = rms_scale(tokens[...].astype(f32), gain_in[...]).astype(bf16).astype(f32)
    halo_copy().wait_recv()
    before = rms_scale(halo[...].astype(f32), gain_in[...]).astype(bf16).astype(f32)
    normed[pl.ds(0, margin), :] = jnp.where(t > 0, before, 0.0)
    where = t * rows + lax.broadcasted_iota(jnp.int32, (rows, gc), 0)

    pool_own().wait()
    for step in range(1, Z):
        pool_z(step, (z + step) % Z).wait_recv()
    for step in range(1, PC):
        pool_plane(step, rp * Y + y).start()
    chain_range(GU, 1, Y)
    for step in range(1, PC):
        pool_plane(step, (rp * Y + y + step) % PC).wait_recv()
    for step in range(1, S):
        for rp_of in range(PR):
            share_copy(step, rp_of, q).start()
    for step in range(1, S):
        for rp_of in range(PR):
            share_copy(step, rp_of, (q + step) % S).wait_recv()
    for group, span in enumerate(pool_spans):
        total = normed[:, group * gc : (group + 1) * gc]
        block = total[margin:]
        reach = 1
        while reach < span:
            total = total + pltpu.roll(total, reach, 0)
            reach *= 2
        gap = (total[margin:] / jnp.minimum(where + 1, span).astype(f32) - block).astype(bf16)
        mixed = jnp.dot(gap, pool_all[group].reshape(gc, gc), preferred_element_type=f32)
        after[:, group * gc : (group + 1) * gc] = mixed.astype(bf16).astype(f32)
    after[...] = tokens[...].astype(f32) + rms_scale(after[...], gain_out[...])
    whole = rms_scale(after[...], gain_ffn[...]).astype(bf16)
    for k in range(F):
        x_all[me, k] = whole[:, k * depth : (k + 1) * depth]
    for step in range(1, C):
        x_copy(step, chip).start()
    for step in range(1, T):
        x_across(step, chip, t).start()

    acc_g[...] = jnp.zeros_like(acc_g)
    acc_u[...] = jnp.zeros_like(acc_u)

    def times(lhs, rhs):
        return jnp.dot(lhs, rhs, preferred_element_type=f32)

    def place_of(g):
        return pl.multiple_of(8 + g // T * (8 + T * rows) + g % T * rows, 8)

    def gate_up_group(origin, g):
        x = x_all[g, origin]
        at = pl.ds(place_of(g), rows)
        acc_g[at, :] += times(x, w_gu[origin, 0])
        acc_u[at, :] += times(x, w_gu[origin, 1])

    def gate_up(origin):
        def body(g, carry):
            gate_up_group(origin, g)
            return carry
        lax.fori_loop(0, G, body, 0)

    early = jnp.where(side > 0, F, Y)
    ahead = Y * (1 + 2 * side)
    y_start(DNS)
    chain_range(GU, Y, early)
    chain_own(DNS)
    chain_range(DNS, 1, Y)
    for back in range(1, C):
        c = (chip + C - back) % C
        x_copy(back, c).wait_recv()
        for step in range(1, T):
            x_across(step, c, t).start()
    for c in range(C):
        for step in range(1, T):
            x_across(step, c, (t + step) % T).wait_recv()

    def gate_up_step(k, carry):
        @pl.when(k >= early)
        def _():
            chain(GU, k)
        gate_up(place(k)[1])
        return carry
    lax.fori_loop(0, F - 1, gate_up_step, 0)
    chain_range(DNS, Y, jnp.minimum(ahead, F - 1))

    @pl.when(F - 1 >= early)
    def _():
        chain(GU, F - 1)

    taps = gate_taps.shape[0]
    window = pl.ds(pl.multiple_of(t * plan.tiles * lanes + plan.first_tile(sub_of(y), t) * lanes, lanes), cols) if plan.joined else slice(None)

    def convolve(acc, taps_ref, g):
        block = acc[pl.ds(pl.multiple_of(place_of(g) - 8, 8), rows + 8), :]
        total = taps_ref[taps - 1 : taps, window] * block[8:]
        for back in range(1, taps):
            total = total + taps_ref[taps - 1 - back : taps - back, window] * pltpu.roll(block, back, 0)[8:]
        return total

    def activate(c):
        def body(t_from, carry):
            g = c * T + t_from
            gate_up_group(place(F - 1)[1], g)
            hidden[g] = (gelu(convolve(acc_g, gate_taps, g)) * convolve(acc_u, up_taps, g)).astype(bf16)
            return carry
        lax.fori_loop(0, T, body, 0)

    def multiply(block, c, h):
        for step in range(1, T):
            t_to = (t + step) % T
            product = jnp.dot(hidden[c * T + t_to], w_d[block, :, part(h)], preferred_element_type=f32)
            partial[block, t_to, c, :, part(h)] = product.astype(bf16)
            s_copy(step, block, t, c, h).start()
        product = jnp.dot(hidden[c * T + t], w_d[block, :, part(h)], preferred_element_type=f32)
        partial[block, t, c, :, part(h)] = product.astype(bf16)

    def add_up(block, c, h):
        for back in range(1, T):
            s_copy(back, block, (t + back) % T, c, h).wait_recv()
        total = partial[block, t, c, :, part(h)].astype(f32)
        for back in range(1, T):
            total = total + swapped[block, T - 1 - back, c, :, part(h)].astype(f32)
        summed[block, c, :, part(h)] = total.astype(bf16)

        @pl.when(c != chip)
        def _():
            p_copy((c + C - chip) % C, block, chip, h).start()

        @pl.when(c == chip)
        def _():
            got[block, chip, :, part(h)] = summed[block, chip, :, part(h)]

    def down(block, h=None, before=None):
        def body(i, carry):
            if before is not None:
                before((chip + 1 + i) % C)
            multiply(block, (chip + 1 + i) % C, h)

            @pl.when(i > 0)
            def _():
                add_up(block, (chip + i) % C, h)
            return carry
        lax.fori_loop(0, C, body, 0)
        add_up(block, chip, h)

    def down_step(k, carry):
        @pl.when(k >= ahead)
        def _():
            chain(DNS, k)
        down(place(k)[1])
        return carry

    if F > 1:
        down(place(0)[1], before=activate)
    else:
        lax.fori_loop(0, C, lambda c, carry: (activate(c), carry)[1], 0)
    lax.fori_loop(1, F - 1, down_step, 0)
    for h in range(H):
        if F > Y:
            chain((DNS[h],), F - 1)
        down(last_block(y), h)

    def finish(block, carry):
        for step in range(1, C):
            @pl.when(block != last_block((chip + step) % C % Y))
            def _():
                p_copy(step, block, (chip + step) % C).wait_recv()
        return carry

    lax.fori_loop(0, F, finish, 0)
    for step in range(1, C):
        for h in range(H):
            c_from = (chip + step) % C
            p_copy(step, last_block(c_from % Y), c_from, h).wait_recv()
    for k in range(F):
        total = got[k, 0].astype(f32)
        for c in range(1, C):
            total = total + got[k, c].astype(f32)
        normed[pl.ds(0, rows), k * depth : (k + 1) * depth] = total
    out[...] = (after[...] + rms_scale(normed[pl.ds(0, rows), :], gain_last[...])).astype(bf16)

    halo_copy().wait_send()
    for step in range(1, Z):
        pool_z(step, z).wait_send()
    for step in range(1, PC):
        pool_plane(step, rp * Y + y).wait_send()
    for step in range(1, S):
        for rp_of in range(PR):
            share_copy(step, rp_of, q).wait_send()
    for step in range(1, C):
        x_copy(step, chip).wait_send()
    for step in range(1, T):
        for c in range(C):
            x_across(step, c, t).wait_send()
    for step in range(1, Y):
        by_size((y + step) % Y, lambda size: [y_copy(kind, step, size).wait_send() for kind in kinds])

    def all_ended(size):
        for kind in kinds:
            def ended(origin, carry):
                @pl.when((origin // Y <= z) & (z + 1 < Z))
                def _():
                    chain_copy(kind, origin, 1, size).wait_send()

                @pl.when((origin // Y >= z) & (z > 0))
                def _():
                    chain_copy(kind, origin, -1, size).wait_send()
                return carry
            lax.fori_loop(0, F, ended, 0)
    by_size(y, all_ended)

    def sent(block, carry):
        @pl.when(block != last_block(y))
        def _():
            for step in range(1, T):
                for c in range(C):
                    s_copy(step, block, t, c).wait_send()
            for step in range(1, C):
                p_copy(step, block, chip).wait_send()
        return carry
    lax.fori_loop(0, F, sent, 0)
    for h in range(H):
        for step in range(1, T):
            for c in range(C):
                s_copy(step, last_block(y), t, c, h).wait_send()
        for step in range(1, C):
            p_copy(step, last_block(y), chip, h).wait_send()


def solution(mesh):
    def shards(tokens, gain_in, pool, gain_out, gain_ffn, gate_w, up_w, gate_taps, up_taps, down_w, gain_last):
        rows, width = tokens.shape
        depth, columns = gate_w.shape
        plan = Plan(mesh, depth, width, columns)
        F, G, T, Y, Z, cols = plan.F, plan.G, plan.T, plan.Y, plan.Z, plan.cols
        groups, gc = pool.shape[0], pool.shape[2]
        C = G // T
        gt, ut = gate_taps, up_taps
        if not plan.joined:
            gt, ut = (lax.dynamic_slice_in_dim(v, lax.axis_index("tp") * columns, columns, 1) for v in (gate_taps, up_taps))
        margin = max(pool_spans)
        vmem = pl.BlockSpec(memory_space=pltpu.VMEM)
        dma = pltpu.SemaphoreType.DMA
        S, PR = plan.pool_owners(groups)
        PC = PR * Y
        H = plan.halves(depth)
        K = 2 + H
        V = pltpu.VMEM
        return pl.pallas_call(
            functools.partial(kernel, plan),
            out_shape=pltpu.VMEM((rows, width), bf16),
            in_specs=[pl.BlockSpec(memory_space=pltpu.HBM)] * 11,
            out_specs=vmem,
            scratch_shapes=[
                V((rows, width), bf16), V((1, width), f32), V((1, width), f32), V((1, width), f32), V(gt.shape, f32), V(ut.shape, f32), V((1, width), f32),
                V((margin, width), bf16), V((groups, Z, gc // Z, gc), bf16), V((F, 2, depth, cols), bf16), V((F, cols, depth), bf16),
                V((G, F, rows, depth), bf16), V((margin + rows, width), f32), V((rows, width), f32),
                V((C * (8 + T * rows), cols), f32), V((C * (8 + T * rows), cols), f32), V((G, rows, cols), bf16),
                V((F, T, C, rows, depth), bf16), V((F, max(T - 1, 1), C, rows, depth), bf16), V((F, C, rows, depth), bf16), V((F, C, rows, depth), bf16),
                dma((7,)), dma((K + 1,)), dma((2,)), dma((K, max(Y - 1, 1))), dma((K, F)), dma((K, F)), dma((K, F)),
                dma((max(Z - 1, 1),)), dma((Z,)), dma((max(PC - 1, 1),)), dma((PC,)), dma((max(S - 1, 1), PR)), dma((PR, S)), dma((max(C - 1, 1),)), dma((G,)),
                dma((max(T - 1, 1), C)), dma((F + H, max(T - 1, 1), C)), dma((F + H, T, C)), dma((F + H, max(C - 1, 1))), dma((F + H, C)),
            ],
            compiler_params=pltpu.CompilerParams(has_side_effects=True, collective_id=0, vmem_limit_bytes=54 * 2**20),
            name="layer",
        )(tokens, gain_in[None], pool, gain_out[None], gain_ffn[None], gate_w, up_w, down_w, gt, ut, gain_last[None])

    in_specs = (
        P(("rep", "fs", "tp"), None), P(), P(None, "fs", None), P(), P(),
        P("fs", "tp"), P("fs", "tp"), P(), P(), P("tp", "fs"), P(),
    )
    return jax.shard_map(shards, mesh=mesh, in_specs=in_specs, out_specs=P(("rep", "fs", "tp"), None), check_vma=False)
```

```python
import functools

import jax
import jax.numpy as jnp
from jax import lax
from jax.experimental import pallas as pl
from jax.experimental.pallas import tpu as pltpu
from jax.sharding import PartitionSpec as P

MESH = pl.DeviceIdType.MESH
pool_spans = (2, 4, 8, 16)
rms_eps = 1e-06
lanes = 128
weight_budget = 24 * 2**20
f32 = jnp.float32
bf16 = jnp.bfloat16


def rms_scale(floats, gain):
    return floats * lax.rsqrt(jnp.mean(floats * floats, axis=-1, keepdims=True) + rms_eps) * gain


def gelu(v):
    return 0.5 * v * (1.0 + jnp.tanh(0.7978845608028654 * (v + 0.044715 * v * v * v)))


class Plan:
    def __init__(self, mesh, depth, width, columns):
        self.R, self.F, self.T = mesh.shape["rep"], mesh.shape["fs"], mesh.shape["tp"]
        self.Y = 1
        while 4 * self.Y * self.Y <= self.F:
            self.Y *= 2
        while self.F % self.Y:
            self.Y -= 1
        self.Z = self.F // self.Y
        self.joined = 3 * width * columns * 2 > weight_budget and columns % lanes == 0
        self.n_sub = self.R * self.Y if self.joined else 1
        self.G = self.T * self.n_sub
        self.tiles = columns // lanes
        self.cols = -(-self.tiles // self.n_sub) * lanes if self.joined else columns
        self.small = self.tiles // self.n_sub * lanes if self.joined else columns

    def halves(self, depth):
        return 2 if depth % (2 * lanes) == 0 else 1

    def first_tile(self, sub, t):
        return (sub * self.tiles + self.n_sub // 2 * ((t + 1) % 2)) // self.n_sub

    def pool_owners(self, groups):
        S = min(self.T, groups)
        PR = self.R if self.joined and groups % (self.R * S) == 0 else 1
        return S, PR


def kernel(
    plan, tokens_hbm, gain_in_hbm, pool, gain_out_hbm, gain_ffn_hbm, gate_w, up_w, down_w, gate_taps_hbm, up_taps_hbm, gain_last_hbm, out,
    tokens, gain_in, gain_out, gain_ffn, gate_taps, up_taps, gain_last,
    halo, pool_all, w_gu, w_d, x_all, normed, after, acc_g, acc_u, hidden, partial, swapped, summed, got,
    in_sem, own_sem, halo_sem, y_ss, up_ss, dn_ss, piece_rs, pz_ss, pz_rs, pp_ss, pp_rs, share_ss, share_rs,
    x_ss, x_rs, f_ss, s_ss, s_rs, p_ss, p_rs,
):
    R, F, T, Y, Z, G, cols = plan.R, plan.F, plan.T, plan.Y, plan.Z, plan.G, plan.cols
    r, f, t = lax.axis_index("rep"), lax.axis_index("fs"), lax.axis_index("tp")
    z, y = f // Y, f % Y
    rows, width = tokens.shape
    depth = width // F
    groups, gc = pool_all.shape[0], pool_all.shape[3]
    slab = gc // F
    S, PR = plan.pool_owners(groups)
    PC = PR * Y
    GS = groups // (S * PR)
    q = t % S
    rp = r if PR > 1 else 0
    margin = halo.shape[0]
    C = G // T
    H = plan.halves(depth)
    half = depth // H
    GA, UP, DN = 0, 1, 2
    GU = (GA, UP)
    DNS = tuple(range(DN, DN + H))
    kinds = GU + DNS
    POOL = DN + H

    chip = r * Y + y if plan.joined else 0
    me = chip * T + t

    def peer(step):
        to = (chip + step) % C
        return {"rep": to // Y, "fs": z * Y + to % Y}

    def sub_of(y_to):
        return r * Y + y_to if plan.joined else 0

    def by_size(y_to, run):
        if plan.small == cols:
            run(cols)
            return
        tiles = plan.first_tile(sub_of(y_to) + 1, t) - plan.first_tile(sub_of(y_to), t)

        @pl.when(tiles * lanes == cols)
        def _():
            run(cols)

        @pl.when(tiles * lanes != cols)
        def _():
            run(plan.small)

    def columns_of(y_to, size):
        if not plan.joined:
            return pl.ds(0, size)
        return pl.ds(pl.multiple_of(plan.first_tile(sub_of(y_to), t) * lanes, lanes), size)

    def part(h):
        return pl.ds(0, depth) if h is None else pl.ds(h * half, half)

    def slot(kind, origin, size):
        if kind in DNS:
            return w_d.at[origin, pl.ds(0, size), part(kind - DN)]
        return w_gu.at[origin, kind - GA, :, pl.ds(0, size)]

    def source(kind, y_to, size):
        if kind in DNS:
            return down_w.at[columns_of(y_to, size), part(kind - DN)]
        return (gate_w, up_w)[kind - GA].at[:, columns_of(y_to, size)]

    def pool_groups(rp_of, q_of):
        return pl.ds((rp_of * S + q_of) * GS, GS)

    def pool_rows(y_of):
        return pl.ds(pl.multiple_of(y_of * slab, slab), slab)

    def pool_own():
        return pltpu.make_async_copy(
            pool.at[pool_groups(rp, q)], pool_all.at[pool_groups(rp, q), z, pool_rows(y)], own_sem.at[POOL])

    def pool_z(step, z_from):
        return pltpu.make_async_remote_copy(
            src_ref=pool.at[pool_groups(rp, q)], dst_ref=pool_all.at[pool_groups(rp, q), z_from, pool_rows(y)],
            send_sem=pz_ss.at[step - 1], recv_sem=pz_rs.at[z_from],
            device_id={"fs": (z + step) % Z * Y + y}, device_id_type=MESH)

    def pool_plane(step, from_pc):
        block = pool_all.at[pool_groups(from_pc // Y, q), :, pool_rows(from_pc % Y)]
        to = (rp * Y + y + step) % PC
        device = {"fs": z * Y + to % Y}
        if PR > 1:
            device["rep"] = to // Y
        return pltpu.make_async_remote_copy(
            src_ref=block, dst_ref=block, send_sem=pp_ss.at[step - 1], recv_sem=pp_rs.at[from_pc],
            device_id=device, device_id_type=MESH)

    def share_copy(step, rp_of, q_from):
        block = pool_all.at[pool_groups(rp_of, q_from)]
        return pltpu.make_async_remote_copy(
            src_ref=block, dst_ref=block, send_sem=share_ss.at[step - 1, rp_of], recv_sem=share_rs.at[rp_of, q_from],
            device_id={"tp": t - q + (q + step) % S}, device_id_type=MESH)

    def own_copy(kind, size):
        return pltpu.make_async_copy(source(kind, y, size), slot(kind, f, size), own_sem.at[kind])

    def y_copy(kind, step, size):
        y_to = (y + step) % Y
        return pltpu.make_async_remote_copy(
            src_ref=source(kind, y_to, size), dst_ref=slot(kind, f, size), send_sem=y_ss.at[kind, step - 1],
            recv_sem=piece_rs.at[kind, f], device_id={"fs": z * Y + y_to}, device_id_type=MESH)

    def chain_copy(kind, origin, dz, size):
        block = slot(kind, origin, size)
        return pltpu.make_async_remote_copy(
            src_ref=block, dst_ref=block, send_sem=(up_ss if dz > 0 else dn_ss).at[kind, origin],
            recv_sem=piece_rs.at[kind, origin], device_id={"fs": (z + dz) * Y + y}, device_id_type=MESH)

    def pass_on(kind, origin, z0, size):
        @pl.when((z0 <= z) & (z + 1 < Z))
        def _():
            chain_copy(kind, origin, 1, size).start()

        @pl.when((z0 >= z) & (z > 0))
        def _():
            chain_copy(kind, origin, -1, size).start()

    def y_start(kinds_now):
        for step in range(1, Y):
            by_size((y + step) % Y, lambda size: [y_copy(kind, step, size).start() for kind in kinds_now])

    side = jnp.minimum(z, Z - 1 - z)

    def place(k):
        j = k // Y
        near = jnp.where(j % 2 == 1, z - (j + 1) // 2, z + j // 2)
        far = jnp.where(2 * z <= Z - 1, j, Z - 1 - j)
        z0 = jnp.where(j <= 2 * side, near, far)
        return z0, z0 * Y + (y + k % Y) % Y

    def chain(kinds_now, k):
        z0, origin = place(k)

        def run(size):
            for kind in kinds_now:
                chain_copy(kind, origin, 1, size).wait_recv()
                pass_on(kind, origin, z0, size)
        by_size(y, run)

    def chain_own(kinds_now):
        def run(size):
            for kind in kinds_now:
                own_copy(kind, size).wait()
                pass_on(kind, f, z, size)
        by_size(y, run)

    def chain_range(kinds_now, first, last):
        def body(k, carry):
            chain(kinds_now, k)
            return carry
        lax.fori_loop(first, last, body, 0)

    def halo_copy():
        return pltpu.make_async_remote_copy(
            src_ref=tokens_hbm.at[pl.ds(rows - margin, margin)], dst_ref=halo, send_sem=halo_sem.at[0],
            recv_sem=halo_sem.at[1], device_id={"tp": (t + 1) % T}, device_id_type=MESH)

    def x_copy(step, c_from):
        g = c_from * T + t
        return pltpu.make_async_remote_copy(
            src_ref=x_all.at[g], dst_ref=x_all.at[g], send_sem=x_ss.at[step - 1],
            recv_sem=x_rs.at[g], device_id=peer(step), device_id_type=MESH)

    def x_across(step, c, t_from):
        g = c * T + t_from
        return pltpu.make_async_remote_copy(
            src_ref=x_all.at[g], dst_ref=x_all.at[g], send_sem=f_ss.at[step - 1, c],
            recv_sem=x_rs.at[g], device_id={"tp": (t + step) % T}, device_id_type=MESH)

    def s_copy(step, turn, block, t_from, c, h=None):
        t_to = (t + step) % T
        window = (slice(None) if c is None else c, slice(None), part(h))
        at = 0 if c is None else c
        return pltpu.make_async_remote_copy(
            src_ref=partial.at[(block, t_to) + window], dst_ref=swapped.at[(block, step - 1) + window],
            send_sem=s_ss.at[turn % 2, step - 1, at], recv_sem=s_rs.at[turn % 2, t_from, at],
            device_id={"tp": t_to}, device_id_type=MESH)

    def p_copy(step, block, c_from, h=None):
        return pltpu.make_async_remote_copy(
            src_ref=summed.at[block, (chip + step) % C, :, part(h)], dst_ref=got.at[block, c_from, :, part(h)],
            send_sem=p_ss.at[block, step - 1], recv_sem=p_rs.at[block, c_from],
            device_id=peer(step), device_id_type=MESH)

    def last_block(y_of):
        return place(F - 1)[0] * Y + (y_of + (F - 1) % Y) % Y

    staged = [
        pltpu.make_async_copy(source_ref, held, in_sem.at[k]) for k, (source_ref, held) in enumerate((
            (tokens_hbm, tokens), (gain_in_hbm, gain_in), (gain_out_hbm, gain_out), (gain_ffn_hbm, gain_ffn),
            (gate_taps_hbm, gate_taps), (up_taps_hbm, up_taps), (gain_last_hbm, gain_last)))]
    staged[0].start()
    staged[1].start()
    pool_own().start()
    by_size(y, lambda size: [own_copy(kind, size).start() for kind in kinds])
    near = [{"fs": (z + step) % Z * Y + y} for step in range(1, Z)]
    near += [peer(step) for step in range(1, C)] if plan.joined else [{"fs": z * Y + (y + step) % Y} for step in range(1, Y)]
    near += [{"tp": (t + step) % T} for step in range(1, T)]
    barrier = pltpu.get_barrier_semaphore()
    for device in near:
        pl.semaphore_signal(barrier, inc=1, device_id=device, device_id_type=MESH)
    def blank(size):
        if size < cols:
            w_gu[:, :, :, size:cols] = jnp.zeros((F, 2, depth, cols - size), bf16)
            w_d[:, size:cols] = jnp.zeros((F, cols - size, depth), bf16)
    by_size(y, blank)
    pl.semaphore_wait(barrier, len(near))

    for step in range(1, Z):
        pool_z(step, z).start()
    halo_copy().start()
    y_start(GU)
    chain_own(GU)
    for copy in staged[2:]:
        copy.start()
    for copy in staged:
        copy.wait()
    normed[pl.ds(margin, rows), :] = rms_scale(tokens[...].astype(f32), gain_in[...]).astype(bf16).astype(f32)
    halo_copy().wait_recv()
    before = rms_scale(halo[...].astype(f32), gain_in[...]).astype(bf16).astype(f32)
    normed[pl.ds(0, margin), :] = jnp.where(t > 0, before, 0.0)
    where = t * rows + lax.broadcasted_iota(jnp.int32, (rows, gc), 0)

    pool_own().wait()
    for step in range(1, Z):
        pool_z(step, (z + step) % Z).wait_recv()
    for step in range(1, PC):
        pool_plane(step, rp * Y + y).start()
    chain_range(GU, 1, Y)
    for step in range(1, PC):
        pool_plane(step, (rp * Y + y + step) % PC).wait_recv()
    for step in range(1, S):
        for rp_of in range(PR):
            share_copy(step, rp_of, q).start()
    for step in range(1, S):
        for rp_of in range(PR):
            share_copy(step, rp_of, (q + step) % S).wait_recv()
    for group, span in enumerate(pool_spans):
        total = normed[:, group * gc : (group + 1) * gc]
        block = total[margin:]
        reach = 1
        while reach < span:
            total = total + pltpu.roll(total, reach, 0)
            reach *= 2
        gap = (total[margin:] / jnp.minimum(where + 1, span).astype(f32) - block).astype(bf16)
        mixed = jnp.dot(gap, pool_all[group].reshape(gc, gc), preferred_element_type=f32)
        after[:, group * gc : (group + 1) * gc] = mixed.astype(bf16).astype(f32)
    after[...] = tokens[...].astype(f32) + rms_scale(after[...], gain_out[...])
    whole = rms_scale(after[...], gain_ffn[...]).astype(bf16)
    for k in range(F):
        x_all[me, k] = whole[:, k * depth : (k + 1) * depth]
    for step in range(1, C):
        x_copy(step, chip).start()
    for step in range(1, T):
        x_across(step, chip, t).start()

    acc_g[...] = jnp.zeros_like(acc_g)
    acc_u[...] = jnp.zeros_like(acc_u)

    def times(lhs, rhs):
        return jnp.dot(lhs, rhs, preferred_element_type=f32)

    def place_of(g):
        return pl.multiple_of(8 + g // T * (8 + T * rows) + g % T * rows, 8)

    def gate_up_group(origin, g):
        x = x_all[g, origin]
        at = pl.ds(place_of(g), rows)
        acc_g[at, :] += times(x, w_gu[origin, 0])
        acc_u[at, :] += times(x, w_gu[origin, 1])

    def gate_up(origin):
        def body(g, carry):
            gate_up_group(origin, g)
            return carry
        lax.fori_loop(0, G, body, 0)

    early = jnp.where(side > 0, F, Y)
    ahead = Y * (1 + 2 * side)
    y_start(DNS)
    chain_range(GU, Y, early)
    chain_own(DNS)
    chain_range(DNS, 1, Y)
    for back in range(1, C):
        c = (chip + C - back) % C
        x_copy(back, c).wait_recv()
        for step in range(1, T):
            x_across(step, c, t).start()
    for c in range(C):
        for step in range(1, T):
            x_across(step, c, (t + step) % T).wait_recv()

    def gate_up_step(k, carry):
        @pl.when(k >= early)
        def _():
            chain(GU, k)
        gate_up(place(k)[1])
        return carry
    lax.fori_loop(0, F - 1, gate_up_step, 0)
    chain_range(DNS, Y, ahead)

    @pl.when(F - 1 >= early)
    def _():
        chain(GU, F - 1)

    taps = gate_taps.shape[0]
    window = pl.ds(pl.multiple_of(t * plan.tiles * lanes + plan.first_tile(sub_of(y), t) * lanes, lanes), cols) if plan.joined else slice(None)

    def convolve(acc, taps_ref, g):
        block = acc[pl.ds(pl.multiple_of(place_of(g) - 8, 8), rows + 8), :]
        total = taps_ref[taps - 1 : taps, window] * block[8:]
        for back in range(1, taps):
            total = total + taps_ref[taps - 1 - back : taps - back, window] * pltpu.roll(block, back, 0)[8:]
        return total

    def activate(c):
        def last_step(t_from, carry):
            gate_up_group(place(F - 1)[1], c * T + t_from)
            return carry

        def hide(t_from, carry):
            g = c * T + t_from
            hidden[t_from, c] = (gelu(convolve(acc_g, gate_taps, g)) * convolve(acc_u, up_taps, g)).astype(bf16)
            return carry
        lax.fori_loop(0, T, last_step, 0)
        lax.fori_loop(0, T, hide, 0)

    def multiply(block, c):
        def body(i, carry):
            t_to = (t + 1 + i) % T
            partial[block, t_to, c] = jnp.dot(hidden[t_to, c], w_d[block], preferred_element_type=f32).astype(bf16)

            @pl.when(i < T - 1)
            def _():
                s_copy(i + 1, 0, block, t, c).start()
            return carry
        lax.fori_loop(0, T, body, 0)

    def wait_swap(turn, block, c, h):
        for back in range(1, T):
            s_copy(back, turn, block, (t + back) % T, c, h).wait_recv()
            s_copy(back, turn, block, t, c, h).wait_send()

    def add_up(block, c, h):
        total = partial[block, t, c, :, part(h)].astype(f32)
        for back in range(1, T):
            total = total + swapped[block, T - 1 - back, c, :, part(h)].astype(f32)
        summed[block, c, :, part(h)] = total.astype(bf16)

        @pl.when(c != chip)
        def _():
            p_copy((c + C - chip) % C, block, chip, h).start()

        @pl.when(c == chip)
        def _():
            got[block, chip, :, part(h)] = summed[block, chip, :, part(h)]

    lag = min(2, C)

    def down_first(block):
        def body(i, carry):
            activate((chip + 1 + i) % C)
            multiply(block, (chip + 1 + i) % C)

            @pl.when(i >= lag)
            def _():
                wait_swap(0, block, (chip + 1 + i - lag) % C, None)
                add_up(block, (chip + 1 + i - lag) % C, None)
            return carry
        lax.fori_loop(0, C, body, 0)
        for i in range(C - lag, C):
            wait_swap(0, block, (chip + 1 + i) % C, None)
            add_up(block, (chip + 1 + i) % C, None)

    def down_half(turn, block, h):
        def body(i, carry):
            t_to = (t + 1 + i) % T
            product = jnp.dot(hidden[t_to].reshape(C * rows, cols), w_d[block, :, part(h)], preferred_element_type=f32)
            partial[block, t_to, :, :, part(h)] = product.astype(bf16).reshape(C, rows, half)

            @pl.when(i < T - 1)
            def _():
                s_copy(i + 1, turn, block, t, None, h).start()
            return carry
        lax.fori_loop(0, T, body, 0)
        wait_swap(turn, block, None, h)
        for i in range(C):
            add_up(block, (chip + 1 + i) % C, h)

    def down_step(k, carry):
        for h in range(H):
            @pl.when(k >= ahead)
            def _():
                chain((DNS[h],), k)
            down_half(1 + (k - 1) * H + h, place(k)[1], h)
        return carry

    down_first(place(0)[1])
    lax.fori_loop(1, F, down_step, 0)

    halo_copy().wait_send()
    for step in range(1, Z):
        pool_z(step, z).wait_send()
    for step in range(1, PC):
        pool_plane(step, rp * Y + y).wait_send()
    for step in range(1, S):
        for rp_of in range(PR):
            share_copy(step, rp_of, q).wait_send()
    for step in range(1, C):
        x_copy(step, chip).wait_send()
    for step in range(1, T):
        for c in range(C):
            x_across(step, c, t).wait_send()
    for step in range(1, Y):
        by_size((y + step) % Y, lambda size: [y_copy(kind, step, size).wait_send() for kind in kinds])

    def all_ended(size):
        for kind in kinds:
            def ended(origin, carry):
                @pl.when((origin // Y <= z) & (z + 1 < Z))
                def _():
                    chain_copy(kind, origin, 1, size).wait_send()

                @pl.when((origin // Y >= z) & (z > 0))
                def _():
                    chain_copy(kind, origin, -1, size).wait_send()
                return carry
            lax.fori_loop(0, F, ended, 0)
    by_size(y, all_ended)

    def sent(block, carry):
        @pl.when(block != last_block(y))
        def _():
            for step in range(1, C):
                p_copy(step, block, chip).wait_send()
        return carry
    lax.fori_loop(0, F, sent, 0)
    def finish(block, carry):
        for step in range(1, C):
            p_copy(step, block, (chip + step) % C).wait_recv()
        return carry

    lax.fori_loop(0, F, finish, 0)
    for k in range(F):
        total = got[k, 0].astype(f32)
        for c in range(1, C):
            total = total + got[k, c].astype(f32)
        normed[pl.ds(0, rows), k * depth : (k + 1) * depth] = total
    out[...] = (after[...] + rms_scale(normed[pl.ds(0, rows), :], gain_last[...])).astype(bf16)

    for step in range(1, C):
        p_copy(step, last_block(y), chip).wait_send()


def solution(mesh):
    def shards(tokens, gain_in, pool, gain_out, gain_ffn, gate_w, up_w, gate_taps, up_taps, down_w, gain_last):
        rows, width = tokens.shape
        depth, columns = gate_w.shape
        plan = Plan(mesh, depth, width, columns)
        F, G, T, Y, Z, cols = plan.F, plan.G, plan.T, plan.Y, plan.Z, plan.cols
        groups, gc = pool.shape[0], pool.shape[2]
        C = G // T
        gt, ut = gate_taps, up_taps
        if not plan.joined:
            gt, ut = (lax.dynamic_slice_in_dim(v, lax.axis_index("tp") * columns, columns, 1) for v in (gate_taps, up_taps))
        margin = max(pool_spans)
        vmem = pl.BlockSpec(memory_space=pltpu.VMEM)
        dma = pltpu.SemaphoreType.DMA
        S, PR = plan.pool_owners(groups)
        PC = PR * Y
        H = plan.halves(depth)
        K = 2 + H
        V = pltpu.VMEM
        return pl.pallas_call(
            functools.partial(kernel, plan),
            out_shape=pltpu.VMEM((rows, width), bf16),
            in_specs=[pl.BlockSpec(memory_space=pltpu.HBM)] * 11,
            out_specs=vmem,
            scratch_shapes=[
                V((rows, width), bf16), V((1, width), f32), V((1, width), f32), V((1, width), f32), V(gt.shape, f32), V(ut.shape, f32), V((1, width), f32),
                V((margin, width), bf16), V((groups, Z, gc // Z, gc), bf16), V((F, 2, depth, cols), bf16), V((F, cols, depth), bf16),
                V((G, F, rows, depth), bf16), V((margin + rows, width), f32), V((rows, width), f32),
                V((C * (8 + T * rows), cols), f32), V((C * (8 + T * rows), cols), f32), V((T, C, rows, cols), bf16),
                V((F, T, C, rows, depth), bf16), V((F, max(T - 1, 1), C, rows, depth), bf16), V((F, C, rows, depth), bf16), V((F, C, rows, depth), bf16),
                dma((7,)), dma((K + 1,)), dma((2,)), dma((K, max(Y - 1, 1))), dma((K, F)), dma((K, F)), dma((K, F)),
                dma((max(Z - 1, 1),)), dma((Z,)), dma((max(PC - 1, 1),)), dma((PC,)), dma((max(S - 1, 1), PR)), dma((PR, S)), dma((max(C - 1, 1),)), dma((G,)),
                dma((max(T - 1, 1), C)), dma((2, max(T - 1, 1), C)), dma((2, T, C)), dma((F, max(C - 1, 1))), dma((F, C)),
            ],
            compiler_params=pltpu.CompilerParams(has_side_effects=True, collective_id=0, vmem_limit_bytes=54 * 2**20),
            name="layer",
        )(tokens, gain_in[None], pool, gain_out[None], gain_ffn[None], gate_w, up_w, down_w, gt, ut, gain_last[None])

    in_specs = (
        P(("rep", "fs", "tp"), None), P(), P(None, "fs", None), P(), P(),
        P("fs", "tp"), P("fs", "tp"), P(), P(), P("tp", "fs"), P(),
    )
    return jax.shard_map(shards, mesh=mesh, in_specs=in_specs, out_specs=P(("rep", "fs", "tp"), None), check_vma=False)
```

```python
import functools

import jax
import jax.numpy as jnp
from jax import lax
from jax.experimental import pallas as pl
from jax.experimental.pallas import tpu as pltpu
from jax.sharding import PartitionSpec as P

MESH = pl.DeviceIdType.MESH
pool_spans = (2, 4, 8, 16)
rms_eps = 1e-06
lanes = 128
weight_budget = 24 * 2**20
f32 = jnp.float32
bf16 = jnp.bfloat16


def rms_scale(floats, gain):
    return floats * lax.rsqrt(jnp.mean(floats * floats, axis=-1, keepdims=True) + rms_eps) * gain


def gelu(v):
    return 0.5 * v * (1.0 + jnp.tanh(0.7978845608028654 * (v + 0.044715 * v * v * v)))


class Plan:
    def __init__(self, mesh, depth, width, columns):
        self.R, self.F, self.T = mesh.shape["rep"], mesh.shape["fs"], mesh.shape["tp"]
        self.Y = 1
        while 4 * self.Y * self.Y <= self.F:
            self.Y *= 2
        while self.F % self.Y:
            self.Y -= 1
        self.Z = self.F // self.Y
        self.joined = 3 * width * columns * 2 > weight_budget and columns % lanes == 0
        self.n_sub = self.R * self.Y if self.joined else 1
        self.G = self.T * self.n_sub
        self.tiles = columns // lanes
        self.cols = -(-self.tiles // self.n_sub) * lanes if self.joined else columns
        self.small = self.tiles // self.n_sub * lanes if self.joined else columns

    def halves(self, depth):
        return 2 if depth % (2 * lanes) == 0 else 1

    def first_tile(self, sub, t):
        return (sub * self.tiles + self.n_sub // 2 * ((t + 1) % 2)) // self.n_sub

    def pool_owners(self, groups):
        S = min(self.T, groups)
        PR = self.R if self.joined and groups % (self.R * S) == 0 else 1
        return S, PR


def kernel(
    plan, tokens_hbm, gain_in_hbm, pool, gain_out_hbm, gain_ffn_hbm, gate_w, up_w, down_w, gate_taps_hbm, up_taps_hbm, gain_last_hbm, out,
    tokens, gain_in, gain_out, gain_ffn, gate_taps, up_taps, gain_last,
    halo, pool_all, w_gu, w_d, x_all, normed, after, acc_g, acc_u, hidden, partial, swapped, summed, got,
    in_sem, own_sem, halo_sem, y_ss, up_ss, dn_ss, piece_rs, pz_ss, pz_rs, pp_ss, pp_rs, share_ss, share_rs,
    x_ss, x_rs, f_ss, s_ss, s_rs, p_ss, p_rs,
):
    R, F, T, Y, Z, G, cols = plan.R, plan.F, plan.T, plan.Y, plan.Z, plan.G, plan.cols
    r, f, t = lax.axis_index("rep"), lax.axis_index("fs"), lax.axis_index("tp")
    z, y = f // Y, f % Y
    rows, width = tokens.shape
    depth = width // F
    groups, gc = pool_all.shape[0], pool_all.shape[3]
    slab = gc // F
    S, PR = plan.pool_owners(groups)
    PC = PR * Y
    GS = groups // (S * PR)
    q = t % S
    rp = r if PR > 1 else 0
    margin = halo.shape[0]
    C = G // T
    H = plan.halves(depth)
    half = depth // H
    GA, UP, DN = 0, 1, 2
    GU = (GA, UP)
    DNS = tuple(range(DN, DN + H))
    kinds = GU + DNS
    POOL = DN + H

    chip = r * Y + y if plan.joined else 0
    me = chip * T + t

    def peer(step):
        to = (chip + step) % C
        return {"rep": to // Y, "fs": z * Y + to % Y}

    def sub_of(y_to):
        return r * Y + y_to if plan.joined else 0

    def by_size(y_to, run):
        if plan.small == cols:
            run(cols)
            return
        tiles = plan.first_tile(sub_of(y_to) + 1, t) - plan.first_tile(sub_of(y_to), t)

        @pl.when(tiles * lanes == cols)
        def _():
            run(cols)

        @pl.when(tiles * lanes != cols)
        def _():
            run(plan.small)

    def columns_of(y_to, size):
        if not plan.joined:
            return pl.ds(0, size)
        return pl.ds(pl.multiple_of(plan.first_tile(sub_of(y_to), t) * lanes, lanes), size)

    def part(h):
        return pl.ds(0, depth) if h is None else pl.ds(h * half, half)

    def slot(kind, origin, size):
        if kind in DNS:
            return w_d.at[origin, pl.ds(0, size), part(kind - DN)]
        return w_gu.at[origin, kind - GA, :, pl.ds(0, size)]

    def source(kind, y_to, size):
        if kind in DNS:
            return down_w.at[columns_of(y_to, size), part(kind - DN)]
        return (gate_w, up_w)[kind - GA].at[:, columns_of(y_to, size)]

    def pool_groups(rp_of, q_of):
        return pl.ds((rp_of * S + q_of) * GS, GS)

    def pool_rows(y_of):
        return pl.ds(pl.multiple_of(y_of * slab, slab), slab)

    def pool_own():
        return pltpu.make_async_copy(
            pool.at[pool_groups(rp, q)], pool_all.at[pool_groups(rp, q), z, pool_rows(y)], own_sem.at[POOL])

    def pool_z(step, z_from):
        return pltpu.make_async_remote_copy(
            src_ref=pool.at[pool_groups(rp, q)], dst_ref=pool_all.at[pool_groups(rp, q), z_from, pool_rows(y)],
            send_sem=pz_ss.at[step - 1], recv_sem=pz_rs.at[z_from],
            device_id={"fs": (z + step) % Z * Y + y}, device_id_type=MESH)

    def pool_plane(step, from_pc):
        block = pool_all.at[pool_groups(from_pc // Y, q), :, pool_rows(from_pc % Y)]
        to = (rp * Y + y + step) % PC
        device = {"fs": z * Y + to % Y}
        if PR > 1:
            device["rep"] = to // Y
        return pltpu.make_async_remote_copy(
            src_ref=block, dst_ref=block, send_sem=pp_ss.at[step - 1], recv_sem=pp_rs.at[from_pc],
            device_id=device, device_id_type=MESH)

    def share_copy(step, rp_of, q_from):
        block = pool_all.at[pool_groups(rp_of, q_from)]
        return pltpu.make_async_remote_copy(
            src_ref=block, dst_ref=block, send_sem=share_ss.at[step - 1, rp_of], recv_sem=share_rs.at[rp_of, q_from],
            device_id={"tp": t - q + (q + step) % S}, device_id_type=MESH)

    def own_copy(kind, size):
        return pltpu.make_async_copy(source(kind, y, size), slot(kind, f, size), own_sem.at[kind])

    def y_copy(kind, step, size):
        y_to = (y + step) % Y
        return pltpu.make_async_remote_copy(
            src_ref=source(kind, y_to, size), dst_ref=slot(kind, f, size), send_sem=y_ss.at[kind, step - 1],
            recv_sem=piece_rs.at[kind, f], device_id={"fs": z * Y + y_to}, device_id_type=MESH)

    def chain_copy(kind, origin, dz, size):
        block = slot(kind, origin, size)
        return pltpu.make_async_remote_copy(
            src_ref=block, dst_ref=block, send_sem=(up_ss if dz > 0 else dn_ss).at[kind],
            recv_sem=piece_rs.at[kind, origin], device_id={"fs": (z + dz) * Y + y}, device_id_type=MESH)

    def pass_on(kind, origin, z0, size):
        @pl.when((z0 <= z) & (z + 1 < Z))
        def _():
            chain_copy(kind, origin, 1, size).start()

        @pl.when((z0 >= z) & (z > 0))
        def _():
            chain_copy(kind, origin, -1, size).start()

    def y_start(kinds_now):
        for step in range(1, Y):
            by_size((y + step) % Y, lambda size: [y_copy(kind, step, size).start() for kind in kinds_now])

    side = jnp.minimum(z, Z - 1 - z)

    def place(k):
        j = k // Y
        near = jnp.where(j % 2 == 1, z - (j + 1) // 2, z + j // 2)
        far = jnp.where(2 * z <= Z - 1, j, Z - 1 - j)
        z0 = jnp.where(j <= 2 * side, near, far)
        return z0, z0 * Y + (y + k % Y) % Y

    def chain(kinds_now, k):
        z0, origin = place(k)

        def run(size):
            for kind in kinds_now:
                chain_copy(kind, origin, 1, size).wait_recv()
                pass_on(kind, origin, z0, size)
        by_size(y, run)

    def chain_own(kinds_now):
        def run(size):
            for kind in kinds_now:
                own_copy(kind, size).wait()
                pass_on(kind, f, z, size)
        by_size(y, run)

    def chain_range(kinds_now, first, last):
        def body(k, carry):
            chain(kinds_now, k)
            return carry
        lax.fori_loop(first, last, body, 0)

    def halo_copy():
        return pltpu.make_async_remote_copy(
            src_ref=tokens_hbm.at[pl.ds(rows - margin, margin)], dst_ref=halo, send_sem=halo_sem.at[0],
            recv_sem=halo_sem.at[1], device_id={"tp": (t + 1) % T}, device_id_type=MESH)

    def x_copy(step, c_from):
        g = c_from * T + t
        return pltpu.make_async_remote_copy(
            src_ref=x_all.at[g], dst_ref=x_all.at[g], send_sem=x_ss.at[step - 1],
            recv_sem=x_rs.at[g], device_id=peer(step), device_id_type=MESH)

    def x_across(step, c, t_from):
        g = c * T + t_from
        return pltpu.make_async_remote_copy(
            src_ref=x_all.at[g], dst_ref=x_all.at[g], send_sem=f_ss.at[step - 1, c],
            recv_sem=x_rs.at[g], device_id={"tp": (t + step) % T}, device_id_type=MESH)

    def s_copy(step, turn, block, t_from, c, h=None):
        t_to = (t + step) % T
        window = (slice(None) if c is None else c, slice(None), part(h))
        at = turn % 2 * C if c is None else c
        return pltpu.make_async_remote_copy(
            src_ref=partial.at[(block, t_to) + window], dst_ref=swapped.at[(block, step - 1) + window],
            send_sem=s_ss.at[step - 1, at], recv_sem=s_rs.at[t_from, at],
            device_id={"tp": t_to}, device_id_type=MESH)

    def p_copy(step, block, c_from, h=None):
        return pltpu.make_async_remote_copy(
            src_ref=summed.at[block, (chip + step) % C, :, part(h)], dst_ref=got.at[block, c_from, :, part(h)],
            send_sem=p_ss.at[step - 1], recv_sem=p_rs.at[block, c_from],
            device_id=peer(step), device_id_type=MESH)

    staged = [
        pltpu.make_async_copy(source_ref, held, in_sem.at[k]) for k, (source_ref, held) in enumerate((
            (tokens_hbm, tokens), (gain_in_hbm, gain_in), (gain_out_hbm, gain_out), (gain_ffn_hbm, gain_ffn),
            (gate_taps_hbm, gate_taps), (up_taps_hbm, up_taps), (gain_last_hbm, gain_last)))]
    staged[0].start()
    staged[1].start()
    pool_own().start()
    by_size(y, lambda size: [own_copy(kind, size).start() for kind in kinds])
    near = [{"fs": (z + step) % Z * Y + y} for step in range(1, Z)]
    near += [peer(step) for step in range(1, C)] if plan.joined else [{"fs": z * Y + (y + step) % Y} for step in range(1, Y)]
    near += [{"tp": (t + step) % T} for step in range(1, T)]
    barrier = pltpu.get_barrier_semaphore()
    for device in near:
        pl.semaphore_signal(barrier, inc=1, device_id=device, device_id_type=MESH)
    def blank(size):
        if size < cols:
            w_gu[:, :, :, size:cols] = jnp.zeros((F, 2, depth, cols - size), bf16)
            w_d[:, size:cols] = jnp.zeros((F, cols - size, depth), bf16)
    by_size(y, blank)
    pl.semaphore_wait(barrier, len(near))

    for step in range(1, Z):
        pool_z(step, z).start()
    halo_copy().start()
    y_start(GU)
    chain_own(GU)
    for copy in staged[2:]:
        copy.start()
    for copy in staged:
        copy.wait()
    normed[pl.ds(margin, rows), :] = rms_scale(tokens[...].astype(f32), gain_in[...]).astype(bf16).astype(f32)
    halo_copy().wait_recv()
    before = rms_scale(halo[...].astype(f32), gain_in[...]).astype(bf16).astype(f32)
    normed[pl.ds(0, margin), :] = jnp.where(t > 0, before, 0.0)
    where = t * rows + lax.broadcasted_iota(jnp.int32, (rows, gc), 0)

    pool_own().wait()
    for step in range(1, Z):
        pool_z(step, (z + step) % Z).wait_recv()
    for step in range(1, PC):
        pool_plane(step, rp * Y + y).start()
    chain_range(GU, 1, Y)
    for step in range(1, PC):
        pool_plane(step, (rp * Y + y + step) % PC).wait_recv()
    for step in range(1, S):
        for rp_of in range(PR):
            share_copy(step, rp_of, q).start()
    for step in range(1, S):
        for rp_of in range(PR):
            share_copy(step, rp_of, (q + step) % S).wait_recv()
    for group, span in enumerate(pool_spans):
        total = normed[:, group * gc : (group + 1) * gc]
        block = total[margin:]
        reach = 1
        while reach < span:
            total = total + pltpu.roll(total, reach, 0)
            reach *= 2
        gap = (total[margin:] / jnp.minimum(where + 1, span).astype(f32) - block).astype(bf16)
        mixed = jnp.dot(gap, pool_all[group].reshape(gc, gc), preferred_element_type=f32)
        after[:, group * gc : (group + 1) * gc] = mixed.astype(bf16).astype(f32)
    after[...] = tokens[...].astype(f32) + rms_scale(after[...], gain_out[...])
    whole = rms_scale(after[...], gain_ffn[...]).astype(bf16)
    for k in range(F):
        x_all[me, k] = whole[:, k * depth : (k + 1) * depth]
    for step in range(1, C):
        x_copy(step, chip).start()
    for step in range(1, T):
        x_across(step, chip, t).start()

    acc_g[...] = jnp.zeros_like(acc_g)
    acc_u[...] = jnp.zeros_like(acc_u)

    def times(lhs, rhs):
        return jnp.dot(lhs, rhs, preferred_element_type=f32)

    def place_of(g):
        return pl.multiple_of(8 + g // T * (8 + T * rows) + g % T * rows, 8)

    def gate_up_group(origin, g):
        x = x_all[g, origin]
        at = pl.ds(place_of(g), rows)
        acc_g[at, :] += times(x, w_gu[origin, 0])
        acc_u[at, :] += times(x, w_gu[origin, 1])

    def gate_up(origin):
        def body(g, carry):
            gate_up_group(origin, g)
            return carry
        lax.fori_loop(0, G, body, 0)

    early = jnp.where(side > 0, F, Y)
    ahead = Y * (1 + 2 * side)
    y_start(DNS)
    chain_range(GU, Y, early)
    chain_own(DNS)
    chain_range(DNS, 1, Y)
    for back in range(1, C):
        c = (chip + C - back) % C
        x_copy(back, c).wait_recv()
        for step in range(1, T):
            x_across(step, c, t).start()
    for c in range(C):
        for step in range(1, T):
            x_across(step, c, (t + step) % T).wait_recv()

    def gate_up_step(k, carry):
        @pl.when(k >= early)
        def _():
            chain(GU, k)
        gate_up(place(k)[1])
        return carry
    lax.fori_loop(0, F - 1, gate_up_step, 0)
    chain_range(DNS, Y, ahead)

    @pl.when(F - 1 >= early)
    def _():
        chain(GU, F - 1)

    taps = gate_taps.shape[0]
    window = pl.ds(pl.multiple_of(t * plan.tiles * lanes + plan.first_tile(sub_of(y), t) * lanes, lanes), cols) if plan.joined else slice(None)

    def convolve(acc, taps_ref, g):
        block = acc[pl.ds(pl.multiple_of(place_of(g) - 8, 8), rows + 8), :]
        total = taps_ref[taps - 1 : taps, window] * block[8:]
        for back in range(1, taps):
            total = total + taps_ref[taps - 1 - back : taps - back, window] * pltpu.roll(block, back, 0)[8:]
        return total

    def activate(c):
        def last_step(t_from, carry):
            gate_up_group(place(F - 1)[1], c * T + t_from)
            return carry

        def hide(t_from, carry):
            g = c * T + t_from
            hidden[t_from, c] = (gelu(convolve(acc_g, gate_taps, g)) * convolve(acc_u, up_taps, g)).astype(bf16)
            return carry
        lax.fori_loop(0, T, last_step, 0)
        lax.fori_loop(0, T, hide, 0)

    def multiply(block, c):
        def body(i, carry):
            t_to = (t + 1 + i) % T
            partial[block, t_to, c] = jnp.dot(hidden[t_to, c], w_d[block], preferred_element_type=f32).astype(bf16)

            @pl.when(i < T - 1)
            def _():
                s_copy(i + 1, 0, block, t, c).start()
            return carry
        lax.fori_loop(0, T, body, 0)

    def wait_swap(turn, block, c, h):
        for back in range(1, T):
            s_copy(back, turn, block, (t + back) % T, c, h).wait_recv()
            s_copy(back, turn, block, t, c, h).wait_send()

    def add_up(block, c, h):
        total = partial[block, t, c, :, part(h)].astype(f32)
        for back in range(1, T):
            total = total + swapped[block, T - 1 - back, c, :, part(h)].astype(f32)
        summed[block, c, :, part(h)] = total.astype(bf16)

        @pl.when(c != chip)
        def _():
            p_copy((c + C - chip) % C, block, chip, h).start()

        @pl.when(c == chip)
        def _():
            got[block, chip, :, part(h)] = summed[block, chip, :, part(h)]

    lag = min(2, C)
    spread = [(dr, dy) for dr in range(R) for dy in range(Y)] if plan.joined else [(0, 0)]
    far_first = sorted(spread, key=lambda d: -((d[0] > 0) + (d[1] > 0)))

    def down_first(block):
        def body(i, carry):
            activate((chip + 1 + i) % C)
            multiply(block, (chip + 1 + i) % C)

            @pl.when(i >= lag)
            def _():
                wait_swap(0, block, (chip + 1 + i - lag) % C, None)
                add_up(block, (chip + 1 + i - lag) % C, None)
            return carry
        lax.fori_loop(0, C, body, 0)
        for i in range(C - lag, C):
            wait_swap(0, block, (chip + 1 + i) % C, None)
            add_up(block, (chip + 1 + i) % C, None)

    def down_half(turn, block, h):
        def body(i, carry):
            t_to = (t + 1 + i) % T
            product = jnp.dot(hidden[t_to].reshape(C * rows, cols), w_d[block, :, part(h)], preferred_element_type=f32)
            partial[block, t_to, :, :, part(h)] = product.astype(bf16).reshape(C, rows, half)

            @pl.when(i < T - 1)
            def _():
                s_copy(i + 1, turn, block, t, None, h).start()
            return carry
        lax.fori_loop(0, T, body, 0)
        wait_swap(turn, block, None, h)
        for dr, dy in far_first:
            add_up(block, (r + dr) % R * Y + (y + dy) % Y if plan.joined else 0, h)

    def down_step(k, carry):
        for h in range(H):
            @pl.when(k >= ahead)
            def _():
                chain((DNS[h],), k)
            down_half(1 + (k - 1) * H + h, place(k)[1], h)
        return carry

    down_first(place(0)[1])
    lax.fori_loop(1, F, down_step, 0)

    halo_copy().wait_send()
    for step in range(1, Z):
        pool_z(step, z).wait_send()
    for step in range(1, PC):
        pool_plane(step, rp * Y + y).wait_send()
    for step in range(1, S):
        for rp_of in range(PR):
            share_copy(step, rp_of, q).wait_send()
    for step in range(1, C):
        x_copy(step, chip).wait_send()
    for step in range(1, T):
        for c in range(C):
            x_across(step, c, t).wait_send()
    for step in range(1, Y):
        by_size((y + step) % Y, lambda size: [y_copy(kind, step, size).wait_send() for kind in kinds])

    def every(kind, first, count, size):
        if kind in DNS:
            return w_d.at[pl.ds(first, count), pl.ds(0, size), part(kind - DN)]
        return w_gu.at[pl.ds(first, count), kind - GA, :, pl.ds(0, size)]

    def all_ended(size):
        for layer in range(Z):
            @pl.when(z == layer)
            def _():
                for kind in kinds:
                    for first, count, dz, sem in ((0, layer * Y + Y, 1, up_ss), (layer * Y, F - layer * Y, -1, dn_ss)):
                        if 0 <= layer + dz < Z:
                            block = every(kind, first, count, size)
                            pltpu.make_async_remote_copy(
                                src_ref=block, dst_ref=block, send_sem=sem.at[kind], recv_sem=piece_rs.at[kind, 0],
                                device_id={"fs": (z + dz) * Y + y}, device_id_type=MESH).wait_send()
    by_size(y, all_ended)

    def finish(k, carry):
        block = place(k)[1]
        for step in range(1, C):
            p_copy(step, block, (chip + step) % C).wait_recv()
        total = got[block, 0].astype(f32)
        for c in range(1, C):
            total = total + got[block, c].astype(f32)
        normed[pl.ds(0, rows), pl.ds(pl.multiple_of(block * depth, depth), depth)] = total
        return carry

    lax.fori_loop(0, F, finish, 0)
    out[...] = (after[...] + rms_scale(normed[pl.ds(0, rows), :], gain_last[...])).astype(bf16)

    for step in range(1, C):
        pltpu.make_async_remote_copy(
            src_ref=summed.at[:, (chip + step) % C], dst_ref=got.at[:, chip], send_sem=p_ss.at[step - 1],
            recv_sem=p_rs.at[0, chip], device_id=peer(step), device_id_type=MESH).wait_send()


def solution(mesh):
    def shards(tokens, gain_in, pool, gain_out, gain_ffn, gate_w, up_w, gate_taps, up_taps, down_w, gain_last):
        rows, width = tokens.shape
        depth, columns = gate_w.shape
        plan = Plan(mesh, depth, width, columns)
        F, G, T, Y, Z, cols = plan.F, plan.G, plan.T, plan.Y, plan.Z, plan.cols
        groups, gc = pool.shape[0], pool.shape[2]
        C = G // T
        gt, ut = gate_taps, up_taps
        if not plan.joined:
            gt, ut = (lax.dynamic_slice_in_dim(v, lax.axis_index("tp") * columns, columns, 1) for v in (gate_taps, up_taps))
        margin = max(pool_spans)
        vmem = pl.BlockSpec(memory_space=pltpu.VMEM)
        dma = pltpu.SemaphoreType.DMA
        S, PR = plan.pool_owners(groups)
        PC = PR * Y
        H = plan.halves(depth)
        K = 2 + H
        V = pltpu.VMEM
        return pl.pallas_call(
            functools.partial(kernel, plan),
            out_shape=pltpu.VMEM((rows, width), bf16),
            in_specs=[pl.BlockSpec(memory_space=pltpu.HBM)] * 11,
            out_specs=vmem,
            scratch_shapes=[
                V((rows, width), bf16), V((1, width), f32), V((1, width), f32), V((1, width), f32), V(gt.shape, f32), V(ut.shape, f32), V((1, width), f32),
                V((margin, width), bf16), V((groups, Z, gc // Z, gc), bf16), V((F, 2, depth, cols), bf16), V((F, cols, depth), bf16),
                V((G, F, rows, depth), bf16), V((margin + rows, width), f32), V((rows, width), f32),
                V((C * (8 + T * rows), cols), f32), V((C * (8 + T * rows), cols), f32), V((T, C, rows, cols), bf16),
                V((F, T, C, rows, depth), bf16), V((F, max(T - 1, 1), C, rows, depth), bf16), V((F, C, rows, depth), bf16), V((F, C, rows, depth), bf16),
                dma((7,)), dma((K + 1,)), dma((2,)), dma((K, max(Y - 1, 1))), dma((K,)), dma((K,)), dma((K, F)),
                dma((max(Z - 1, 1),)), dma((Z,)), dma((max(PC - 1, 1),)), dma((PC,)), dma((max(S - 1, 1), PR)), dma((PR, S)), dma((max(C - 1, 1),)), dma((G,)),
                dma((max(T - 1, 1), C)), dma((max(T - 1, 1), C + 1)), dma((T, C + 1)), dma((max(C - 1, 1),)), dma((F, C)),
            ],
            compiler_params=pltpu.CompilerParams(has_side_effects=True, collective_id=0, vmem_limit_bytes=54 * 2**20),
            name="layer",
        )(tokens, gain_in[None], pool, gain_out[None], gain_ffn[None], gate_w, up_w, down_w, gt, ut, gain_last[None])

    in_specs = (
        P(("rep", "fs", "tp"), None), P(), P(None, "fs", None), P(), P(),
        P("fs", "tp"), P("fs", "tp"), P(), P(), P("tp", "fs"), P(),
    )
    return jax.shard_map(shards, mesh=mesh, in_specs=in_specs, out_specs=P(("rep", "fs", "tp"), None), check_vma=False)
```

```python
import functools

import jax
import jax.numpy as jnp
from jax import lax
from jax.experimental import pallas as pl
from jax.experimental.pallas import tpu as pltpu
from jax.sharding import PartitionSpec as P

MESH = pl.DeviceIdType.MESH
pool_spans = (2, 4, 8, 16)
rms_eps = 1e-06
lanes = 128
weight_budget = 24 * 2**20
f32 = jnp.float32
bf16 = jnp.bfloat16


def rms_scale(floats, gain):
    return floats * lax.rsqrt(jnp.mean(floats * floats, axis=-1, keepdims=True) + rms_eps) * gain


def gelu(v):
    return 0.5 * v * (1.0 + jnp.tanh(0.7978845608028654 * (v + 0.044715 * v * v * v)))


class Plan:
    def __init__(self, mesh, depth, width, columns):
        self.R, self.F, self.T = mesh.shape["rep"], mesh.shape["fs"], mesh.shape["tp"]
        self.Y = 1
        while 4 * self.Y * self.Y <= self.F:
            self.Y *= 2
        while self.F % self.Y:
            self.Y -= 1
        self.Z = self.F // self.Y
        self.joined = 3 * width * columns * 2 > weight_budget and columns % lanes == 0
        self.n_sub = self.R * self.Y if self.joined else 1
        self.G = self.T * self.n_sub
        self.tiles = columns // lanes
        self.cols = -(-self.tiles // self.n_sub) * lanes if self.joined else columns
        self.small = self.tiles // self.n_sub * lanes if self.joined else columns

    def halves(self, depth):
        return 2 if depth % (2 * lanes) == 0 else 1

    def first_tile(self, sub, t):
        return (sub * self.tiles + self.n_sub // 2 * ((t + 1) % 2)) // self.n_sub

    def pool_owners(self, groups):
        S = min(self.T, groups)
        PR = self.R if self.joined and groups % (self.R * S) == 0 else 1
        return S, PR


def kernel(
    plan, tokens_hbm, gain_in_hbm, pool, gain_out_hbm, gain_ffn_hbm, gate_w, up_w, down_w, gate_taps_hbm, up_taps_hbm, gain_last_hbm, out,
    tokens, gain_in, gain_out, gain_ffn, gate_taps, up_taps, gain_last,
    halo, pool_all, w_gu, w_d, x_all, normed, after, acc_g, acc_u, hidden, partial, swapped, summed, got,
    in_sem, own_sem, halo_sem, y_ss, up_ss, dn_ss, piece_rs, pz_ss, pz_rs, pp_ss, pp_rs, share_ss, share_rs,
    x_ss, x_rs, f_ss, s_ss, s_rs, p_ss, p_rs,
):
    R, F, T, Y, Z, G, cols = plan.R, plan.F, plan.T, plan.Y, plan.Z, plan.G, plan.cols
    r, f, t = lax.axis_index("rep"), lax.axis_index("fs"), lax.axis_index("tp")
    z, y = f // Y, f % Y
    rows, width = tokens.shape
    depth = width // F
    groups, gc = pool_all.shape[0], pool_all.shape[3]
    slab = gc // F
    S, PR = plan.pool_owners(groups)
    PC = PR * Y
    GS = groups // (S * PR)
    q = t % S
    rp = r if PR > 1 else 0
    margin = halo.shape[0]
    C = G // T
    H = plan.halves(depth)
    half = depth // H
    GA, UP, DN = 0, 1, 2
    GU = (GA, UP)
    DNS = tuple(range(DN, DN + H))
    kinds = GU + DNS
    POOL = DN + H

    chip = r * Y + y if plan.joined else 0
    me = chip * T + t

    def peer(step):
        to = (chip + step) % C
        return {"rep": to // Y, "fs": z * Y + to % Y}

    def sub_of(y_to):
        return r * Y + y_to if plan.joined else 0

    def by_size(y_to, run):
        if plan.small == cols:
            run(cols)
            return
        tiles = plan.first_tile(sub_of(y_to) + 1, t) - plan.first_tile(sub_of(y_to), t)

        @pl.when(tiles * lanes == cols)
        def _():
            run(cols)

        @pl.when(tiles * lanes != cols)
        def _():
            run(plan.small)

    def columns_of(y_to, size):
        if not plan.joined:
            return pl.ds(0, size)
        return pl.ds(pl.multiple_of(plan.first_tile(sub_of(y_to), t) * lanes, lanes), size)

    def part(h):
        return pl.ds(0, depth) if h is None else pl.ds(h * half, half)

    def slot(kind, origin, size):
        if kind in DNS:
            return w_d.at[origin, pl.ds(0, size), part(kind - DN)]
        return w_gu.at[origin, kind - GA, :, pl.ds(0, size)]

    def source(kind, y_to, size):
        if kind in DNS:
            return down_w.at[columns_of(y_to, size), part(kind - DN)]
        return (gate_w, up_w)[kind - GA].at[:, columns_of(y_to, size)]

    def pool_groups(rp_of, q_of):
        return pl.ds((rp_of * S + q_of) * GS, GS)

    def pool_rows(y_of):
        return pl.ds(pl.multiple_of(y_of * slab, slab), slab)

    def pool_own():
        return pltpu.make_async_copy(
            pool.at[pool_groups(rp, q)], pool_all.at[pool_groups(rp, q), z, pool_rows(y)], own_sem.at[POOL])

    def pool_z(step, z_from):
        return pltpu.make_async_remote_copy(
            src_ref=pool.at[pool_groups(rp, q)], dst_ref=pool_all.at[pool_groups(rp, q), z_from, pool_rows(y)],
            send_sem=pz_ss.at[step - 1], recv_sem=pz_rs.at[z_from],
            device_id={"fs": (z + step) % Z * Y + y}, device_id_type=MESH)

    def pool_plane(step, from_pc):
        block = pool_all.at[pool_groups(from_pc // Y, q), :, pool_rows(from_pc % Y)]
        to = (rp * Y + y + step) % PC
        device = {"fs": z * Y + to % Y}
        if PR > 1:
            device["rep"] = to // Y
        return pltpu.make_async_remote_copy(
            src_ref=block, dst_ref=block, send_sem=pp_ss.at[step - 1], recv_sem=pp_rs.at[from_pc],
            device_id=device, device_id_type=MESH)

    def share_copy(step, rp_of, q_from):
        block = pool_all.at[pool_groups(rp_of, q_from)]
        return pltpu.make_async_remote_copy(
            src_ref=block, dst_ref=block, send_sem=share_ss.at[step - 1, rp_of], recv_sem=share_rs.at[rp_of, q_from],
            device_id={"tp": t - q + (q + step) % S}, device_id_type=MESH)

    def own_copy(kind, size):
        return pltpu.make_async_copy(source(kind, y, size), slot(kind, f, size), own_sem.at[kind])

    def y_copy(kind, step, size):
        y_to = (y + step) % Y
        return pltpu.make_async_remote_copy(
            src_ref=source(kind, y_to, size), dst_ref=slot(kind, f, size), send_sem=y_ss.at[kind, step - 1],
            recv_sem=piece_rs.at[kind, f], device_id={"fs": z * Y + y_to}, device_id_type=MESH)

    def chain_copy(kind, origin, dz, size):
        block = slot(kind, origin, size)
        return pltpu.make_async_remote_copy(
            src_ref=block, dst_ref=block, send_sem=(up_ss if dz > 0 else dn_ss).at[kind],
            recv_sem=piece_rs.at[kind, origin], device_id={"fs": (z + dz) * Y + y}, device_id_type=MESH)

    def pass_on(kind, origin, z0, size):
        @pl.when((z0 <= z) & (z + 1 < Z))
        def _():
            chain_copy(kind, origin, 1, size).start()

        @pl.when((z0 >= z) & (z > 0))
        def _():
            chain_copy(kind, origin, -1, size).start()

    def y_start(kinds_now):
        for step in range(1, Y):
            by_size((y + step) % Y, lambda size: [y_copy(kind, step, size).start() for kind in kinds_now])

    side = jnp.minimum(z, Z - 1 - z)

    def place(k):
        j = k // Y
        near = jnp.where(j % 2 == 1, z - (j + 1) // 2, z + j // 2)
        far = jnp.where(2 * z <= Z - 1, j, Z - 1 - j)
        z0 = jnp.where(j <= 2 * side, near, far)
        return z0, z0 * Y + (y + k % Y) % Y

    def chain(kinds_now, k):
        z0, origin = place(k)

        def run(size):
            for kind in kinds_now:
                chain_copy(kind, origin, 1, size).wait_recv()
                pass_on(kind, origin, z0, size)
        by_size(y, run)

    def chain_own(kinds_now):
        def run(size):
            for kind in kinds_now:
                own_copy(kind, size).wait()
                pass_on(kind, f, z, size)
        by_size(y, run)

    def chain_range(kinds_now, first, last):
        def body(k, carry):
            chain(kinds_now, k)
            return carry
        lax.fori_loop(first, last, body, 0)

    def halo_copy():
        return pltpu.make_async_remote_copy(
            src_ref=tokens_hbm.at[pl.ds(rows - margin, margin)], dst_ref=halo, send_sem=halo_sem.at[0],
            recv_sem=halo_sem.at[1], device_id={"tp": (t + 1) % T}, device_id_type=MESH)

    def x_copy(step, c_from):
        g = c_from * T + t
        return pltpu.make_async_remote_copy(
            src_ref=x_all.at[g], dst_ref=x_all.at[g], send_sem=x_ss.at[step - 1],
            recv_sem=x_rs.at[g], device_id=peer(step), device_id_type=MESH)

    def x_across(step, c, t_from):
        g = c * T + t_from
        return pltpu.make_async_remote_copy(
            src_ref=x_all.at[g], dst_ref=x_all.at[g], send_sem=f_ss.at[step - 1, c],
            recv_sem=x_rs.at[g], device_id={"tp": (t + step) % T}, device_id_type=MESH)

    def s_copy(step, turn, block, t_from, c, h=None):
        t_to = (t + step) % T
        window = (slice(None) if c is None else c, slice(None), part(h))
        at = turn % 2 * C if c is None else c
        return pltpu.make_async_remote_copy(
            src_ref=partial.at[(block, t_to) + window], dst_ref=swapped.at[(block, step - 1) + window],
            send_sem=s_ss.at[step - 1, at], recv_sem=s_rs.at[t_from, at],
            device_id={"tp": t_to}, device_id_type=MESH)

    def p_copy(step, block, c_from, h=None):
        return pltpu.make_async_remote_copy(
            src_ref=summed.at[block, (chip + step) % C, :, part(h)], dst_ref=got.at[block, c_from, :, part(h)],
            send_sem=p_ss.at[step - 1], recv_sem=p_rs.at[block, c_from],
            device_id=peer(step), device_id_type=MESH)

    staged = [
        pltpu.make_async_copy(source_ref, held, in_sem.at[k]) for k, (source_ref, held) in enumerate((
            (tokens_hbm, tokens), (gain_in_hbm, gain_in), (gain_out_hbm, gain_out), (gain_ffn_hbm, gain_ffn),
            (gate_taps_hbm, gate_taps), (up_taps_hbm, up_taps), (gain_last_hbm, gain_last)))]
    staged[0].start()
    staged[1].start()
    pool_own().start()
    by_size(y, lambda size: [own_copy(kind, size).start() for kind in kinds])
    near = [{"fs": (z + step) % Z * Y + y} for step in range(1, Z)]
    near += [peer(step) for step in range(1, C)] if plan.joined else [{"fs": z * Y + (y + step) % Y} for step in range(1, Y)]
    near += [{"tp": (t + step) % T} for step in range(1, T)]
    barrier = pltpu.get_barrier_semaphore()
    for device in near:
        pl.semaphore_signal(barrier, inc=1, device_id=device, device_id_type=MESH)
    def blank(size):
        if size < cols:
            w_gu[:, :, :, size:cols] = jnp.zeros((F, 2, depth, cols - size), bf16)
            w_d[:, size:cols] = jnp.zeros((F, cols - size, depth), bf16)
    by_size(y, blank)
    pl.semaphore_wait(barrier, len(near))

    for step in range(1, Z):
        pool_z(step, z).start()
    halo_copy().start()
    y_start(GU)
    chain_own(GU)
    for copy in staged[2:]:
        copy.start()
    for copy in staged:
        copy.wait()
    normed[pl.ds(margin, rows), :] = rms_scale(tokens[...].astype(f32), gain_in[...]).astype(bf16).astype(f32)
    halo_copy().wait_recv()
    before = rms_scale(halo[...].astype(f32), gain_in[...]).astype(bf16).astype(f32)
    normed[pl.ds(0, margin), :] = jnp.where(t > 0, before, 0.0)
    where = t * rows + lax.broadcasted_iota(jnp.int32, (rows, gc), 0)

    pool_own().wait()
    for step in range(1, Z):
        pool_z(step, (z + step) % Z).wait_recv()
    for step in range(1, PC):
        pool_plane(step, rp * Y + y).start()
    chain_range(GU, 1, Y)
    for step in range(1, PC):
        pool_plane(step, (rp * Y + y + step) % PC).wait_recv()
    for step in range(1, S):
        for rp_of in range(PR):
            share_copy(step, rp_of, q).start()
    for step in range(1, S):
        for rp_of in range(PR):
            share_copy(step, rp_of, (q + step) % S).wait_recv()
    for group, span in enumerate(pool_spans):
        total = normed[:, group * gc : (group + 1) * gc]
        block = total[margin:]
        reach = 1
        while reach < span:
            total = total + pltpu.roll(total, reach, 0)
            reach *= 2
        gap = (total[margin:] / jnp.minimum(where + 1, span).astype(f32) - block).astype(bf16)
        mixed = jnp.dot(gap, pool_all[group].reshape(gc, gc), preferred_element_type=f32)
        after[:, group * gc : (group + 1) * gc] = mixed.astype(bf16).astype(f32)
    after[...] = tokens[...].astype(f32) + rms_scale(after[...], gain_out[...])
    whole = rms_scale(after[...], gain_ffn[...]).astype(bf16)
    for k in range(F):
        x_all[me, k] = whole[:, k * depth : (k + 1) * depth]
    for step in range(1, C):
        x_copy(step, chip).start()
    for step in range(1, T):
        x_across(step, chip, t).start()

    acc_g[...] = jnp.zeros_like(acc_g)
    acc_u[...] = jnp.zeros_like(acc_u)

    def times(lhs, rhs):
        return jnp.dot(lhs, rhs, preferred_element_type=f32)

    def place_of(g):
        return pl.multiple_of(8 + g // T * (8 + T * rows) + g % T * rows, 8)

    def gate_up_group(origin, g):
        x = x_all[g, origin]
        at = pl.ds(place_of(g), rows)
        acc_g[at, :] += times(x, w_gu[origin, 0])
        acc_u[at, :] += times(x, w_gu[origin, 1])

    def gate_up(origin):
        def body(g, carry):
            gate_up_group(origin, g)
            return carry
        lax.fori_loop(0, G, body, 0)

    early = jnp.where(side > 0, F, Y)
    ahead = Y * (1 + 2 * side)
    y_start(DNS)
    chain_range(GU, Y, early)
    chain_own(DNS)
    chain_range(DNS, 1, Y)
    for back in range(1, C):
        c = (chip + C - back) % C
        x_copy(back, c).wait_recv()
        for step in range(1, T):
            x_across(step, c, t).start()
    for c in range(C):
        for step in range(1, T):
            x_across(step, c, (t + step) % T).wait_recv()

    def gate_up_step(k, carry):
        @pl.when(k >= early)
        def _():
            chain(GU, k)
        gate_up(place(k)[1])
        return carry
    lax.fori_loop(0, F - 1, gate_up_step, 0)
    chain_range(DNS, Y, ahead)

    @pl.when(F - 1 >= early)
    def _():
        chain(GU, F - 1)

    taps = gate_taps.shape[0]
    window = pl.ds(pl.multiple_of(t * plan.tiles * lanes + plan.first_tile(sub_of(y), t) * lanes, lanes), cols) if plan.joined else slice(None)

    def convolve(acc, taps_ref, g):
        block = acc[pl.ds(pl.multiple_of(place_of(g) - 8, 8), rows + 8), :]
        total = taps_ref[taps - 1 : taps, window] * block[8:]
        for back in range(1, taps):
            total = total + taps_ref[taps - 1 - back : taps - back, window] * pltpu.roll(block, back, 0)[8:]
        return total

    def activate(c):
        def last_step(t_from, carry):
            gate_up_group(place(F - 1)[1], c * T + t_from)
            return carry

        def hide(t_from, carry):
            g = c * T + t_from
            hidden[t_from, c] = (gelu(convolve(acc_g, gate_taps, g)) * convolve(acc_u, up_taps, g)).astype(bf16)
            return carry
        lax.fori_loop(0, T, last_step, 0)
        lax.fori_loop(0, T, hide, 0)

    def multiply(block, c):
        def body(i, carry):
            t_to = (t + 1 + i) % T
            partial[block, t_to, c] = jnp.dot(hidden[t_to, c], w_d[block], preferred_element_type=f32).astype(bf16)

            @pl.when(i < T - 1)
            def _():
                s_copy(i + 1, 0, block, t, c).start()
            return carry
        lax.fori_loop(0, T, body, 0)

    def wait_swap(turn, block, c, h):
        for back in range(1, T):
            s_copy(back, turn, block, (t + back) % T, c, h).wait_recv()
            s_copy(back, turn, block, t, c, h).wait_send()

    def add_up(block, c, h):
        total = partial[block, t, c, :, part(h)].astype(f32)
        for back in range(1, T):
            total = total + swapped[block, T - 1 - back, c, :, part(h)].astype(f32)
        summed[block, c, :, part(h)] = total.astype(bf16)

        @pl.when(c != chip)
        def _():
            p_copy((c + C - chip) % C, block, chip, h).start()

        @pl.when(c == chip)
        def _():
            got[block, chip, :, part(h)] = summed[block, chip, :, part(h)]

    lag = min(2, C)
    spread = [(dr, dy) for dr in range(R) for dy in range(Y)] if plan.joined else [(0, 0)]
    far_first = sorted(spread, key=lambda d: -((d[0] > 0) + (d[1] > 0)))

    def down_first(block):
        def body(i, carry):
            activate((chip + 1 + i) % C)
            multiply(block, (chip + 1 + i) % C)

            @pl.when(i >= lag)
            def _():
                wait_swap(0, block, (chip + 1 + i - lag) % C, None)
                add_up(block, (chip + 1 + i - lag) % C, None)
            return carry
        lax.fori_loop(0, C, body, 0)
        for i in range(C - lag, C):
            wait_swap(0, block, (chip + 1 + i) % C, None)
            add_up(block, (chip + 1 + i) % C, None)

    def down_half(turn, block, h):
        def body(i, carry):
            t_to = (t + 1 + i) % T
            product = jnp.dot(hidden[t_to].reshape(C * rows, cols), w_d[block, :, part(h)], preferred_element_type=f32)
            partial[block, t_to, :, :, part(h)] = product.astype(bf16).reshape(C, rows, half)

            @pl.when(i < T - 1)
            def _():
                s_copy(i + 1, turn, block, t, None, h).start()
            return carry
        lax.fori_loop(0, T, body, 0)
        wait_swap(turn, block, None, h)
        for dr, dy in far_first:
            add_up(block, (r + dr) % R * Y + (y + dy) % Y if plan.joined else 0, h)

    lead = jnp.where(side > 0, jnp.minimum(4, ahead - 1), 0)

    def down_step(k, carry):
        for h in range(H):
            @pl.when((k + lead >= ahead) & (k + lead < F))
            def _():
                chain((DNS[h],), k + lead)
            down_half(1 + (k - 1) * H + h, place(k)[1], h)
        return carry

    down_first(place(0)[1])
    lax.fori_loop(1, F, down_step, 0)

    halo_copy().wait_send()
    for step in range(1, Z):
        pool_z(step, z).wait_send()
    for step in range(1, PC):
        pool_plane(step, rp * Y + y).wait_send()
    for step in range(1, S):
        for rp_of in range(PR):
            share_copy(step, rp_of, q).wait_send()
    for step in range(1, C):
        x_copy(step, chip).wait_send()
    for step in range(1, T):
        for c in range(C):
            x_across(step, c, t).wait_send()
    for step in range(1, Y):
        by_size((y + step) % Y, lambda size: [y_copy(kind, step, size).wait_send() for kind in kinds])

    def every(kind, first, count, size):
        if kind in DNS:
            return w_d.at[pl.ds(first, count), pl.ds(0, size), part(kind - DN)]
        return w_gu.at[pl.ds(first, count), kind - GA, :, pl.ds(0, size)]

    def all_ended(size):
        for layer in range(Z):
            @pl.when(z == layer)
            def _():
                for kind in kinds:
                    for first, count, dz, sem in ((0, layer * Y + Y, 1, up_ss), (layer * Y, F - layer * Y, -1, dn_ss)):
                        if 0 <= layer + dz < Z:
                            block = every(kind, first, count, size)
                            pltpu.make_async_remote_copy(
                                src_ref=block, dst_ref=block, send_sem=sem.at[kind], recv_sem=piece_rs.at[kind, 0],
                                device_id={"fs": (z + dz) * Y + y}, device_id_type=MESH).wait_send()
    by_size(y, all_ended)

    def finish(k, carry):
        block = place(k)[1]
        for step in range(1, C):
            p_copy(step, block, (chip + step) % C).wait_recv()
        total = got[block, 0].astype(f32)
        for c in range(1, C):
            total = total + got[block, c].astype(f32)
        normed[pl.ds(0, rows), pl.ds(pl.multiple_of(block * depth, depth), depth)] = total
        return carry + jnp.sum(total * total, axis=-1, keepdims=True)

    squares = lax.fori_loop(0, F, finish, jnp.zeros((rows, 1), f32))
    out[...] = (after[...] + normed[pl.ds(0, rows), :] * lax.rsqrt(squares / width + rms_eps) * gain_last[...]).astype(bf16)

    for step in range(1, C):
        pltpu.make_async_remote_copy(
            src_ref=summed.at[:, (chip + step) % C], dst_ref=got.at[:, chip], send_sem=p_ss.at[step - 1],
            recv_sem=p_rs.at[0, chip], device_id=peer(step), device_id_type=MESH).wait_send()


def solution(mesh):
    def shards(tokens, gain_in, pool, gain_out, gain_ffn, gate_w, up_w, gate_taps, up_taps, down_w, gain_last):
        rows, width = tokens.shape
        depth, columns = gate_w.shape
        plan = Plan(mesh, depth, width, columns)
        F, G, T, Y, Z, cols = plan.F, plan.G, plan.T, plan.Y, plan.Z, plan.cols
        groups, gc = pool.shape[0], pool.shape[2]
        C = G // T
        gt, ut = gate_taps, up_taps
        if not plan.joined:
            gt, ut = (lax.dynamic_slice_in_dim(v, lax.axis_index("tp") * columns, columns, 1) for v in (gate_taps, up_taps))
        margin = max(pool_spans)
        vmem = pl.BlockSpec(memory_space=pltpu.VMEM)
        dma = pltpu.SemaphoreType.DMA
        S, PR = plan.pool_owners(groups)
        PC = PR * Y
        H = plan.halves(depth)
        K = 2 + H
        V = pltpu.VMEM
        return pl.pallas_call(
            functools.partial(kernel, plan),
            out_shape=pltpu.VMEM((rows, width), bf16),
            in_specs=[pl.BlockSpec(memory_space=pltpu.HBM)] * 11,
            out_specs=vmem,
            scratch_shapes=[
                V((rows, width), bf16), V((1, width), f32), V((1, width), f32), V((1, width), f32), V(gt.shape, f32), V(ut.shape, f32), V((1, width), f32),
                V((margin, width), bf16), V((groups, Z, gc // Z, gc), bf16), V((F, 2, depth, cols), bf16), V((F, cols, depth), bf16),
                V((G, F, rows, depth), bf16), V((margin + rows, width), f32), V((rows, width), f32),
                V((C * (8 + T * rows), cols), f32), V((C * (8 + T * rows), cols), f32), V((T, C, rows, cols), bf16),
                V((F, T, C, rows, depth), bf16), V((F, max(T - 1, 1), C, rows, depth), bf16), V((F, C, rows, depth), bf16), V((F, C, rows, depth), bf16),
                dma((7,)), dma((K + 1,)), dma((2,)), dma((K, max(Y - 1, 1))), dma((K,)), dma((K,)), dma((K, F)),
                dma((max(Z - 1, 1),)), dma((Z,)), dma((max(PC - 1, 1),)), dma((PC,)), dma((max(S - 1, 1), PR)), dma((PR, S)), dma((max(C - 1, 1),)), dma((G,)),
                dma((max(T - 1, 1), C)), dma((max(T - 1, 1), C + 1)), dma((T, C + 1)), dma((max(C - 1, 1),)), dma((F, C)),
            ],
            compiler_params=pltpu.CompilerParams(has_side_effects=True, collective_id=0, vmem_limit_bytes=54 * 2**20),
            name="layer",
        )(tokens, gain_in[None], pool, gain_out[None], gain_ffn[None], gate_w, up_w, down_w, gt, ut, gain_last[None])

    in_specs = (
        P(("rep", "fs", "tp"), None), P(), P(None, "fs", None), P(), P(),
        P("fs", "tp"), P("fs", "tp"), P(), P(), P("tp", "fs"), P(),
    )
    return jax.shard_map(shards, mesh=mesh, in_specs=in_specs, out_specs=P(("rep", "fs", "tp"), None), check_vma=False)
```
